512 devices in a mesh: sp: 16 (over y, x), tp: 32 (over z, core).
Axes of the slice: x: 4, y: 4, z: 16, core: 2. Of those that a mesh axis runs over, the one named last changes fastest.
Arguments:
- tokens: bfloat16 [8, 49152, 2048], P(None, ('sp', 'tp')), may hold values from -13 to 13
- in_gain: float32 [2048], replicated, may hold values from 0.1 to 1.9
- w_key: bfloat16 [2048, 512], P('tp'), may hold values from -0.125 to 0.125
- w_value: bfloat16 [2048, 512], P('tp'), may hold values from -0.125 to 0.125
- k_gain: float32 [128], replicated, may hold values from 0.1 to 1.9
- new_query: bfloat16 [8, 1024], replicated, may hold values from -6 to 6
- q_gain: float32 [128], replicated, may hold values from 0.1 to 1.9
- stick_bias: float32 [8], replicated, may hold values from -13 to -3
Outputs:
- key_cache: bfloat16 [32, 49152, 128], P('tp', 'sp')
- value_cache: bfloat16 [32, 49152, 128], P('tp', 'sp')
- read_out: float32 [32, 256], P('tp')
The draws below stay inside these ranges and needn't reach their ends.
All inputs are finite; a program needn't handle non-finite values.
Results may differ from the reference program's by a relative error of at most 0.005.
Values may be sent and summed in bfloat16 or wider, within the bound.
A program may use at most 64 MiB of HBM per device.

```python
import jax
import jax.numpy as jnp
from jax import lax

D = 2048
HEADS = 8
KVH = 4
HD = 128
SEQS = 8
LENGTH = 49152


def draw_tokens(key, part):
    noise_key, common_key, level_key = jax.random.split(jax.random.fold_in(key, 11), 3)
    block_count = LENGTH // 32
    noise_part = jnp.clip(jax.random.normal(noise_key, (SEQS, LENGTH, D), jnp.float32), -5.0, 5.0)
    levels = jnp.exp(jax.random.uniform(level_key, (SEQS, block_count, 1), jnp.float32, -1.2, 0.9))
    common = jnp.clip(jax.random.normal(common_key, (SEQS, 1, D), jnp.float32), -3.0, 3.0)
    levels = jnp.repeat(levels, 32, axis=1)
    return (noise_part + levels * common).astype(jnp.bfloat16)


def draw_stick_bias(key, part):
    order_key, fast_key, slow_key = jax.random.split(jax.random.fold_in(key, 23), 3)
    chain = jnp.log(jnp.float32(LENGTH))
    slow_bias = -chain + jax.random.uniform(slow_key, (HEADS,), jnp.float32, -1.5, 0.0)
    fast_bias = jax.random.uniform(fast_key, (HEADS,), jnp.float32, -4.5, -3.5)
    ranking = jax.random.permutation(order_key, HEADS)
    is_fast = ranking < HEADS // 2
    return jnp.where(is_fast, fast_bias, slow_bias)


def steps_of(own_key, shape, pieces, least, high):
    loudness = 1.0
    for axis_at, parts in pieces:
        heights = jax.random.uniform(jax.random.fold_in(jax.random.fold_in(own_key, 6), axis_at), (parts,), jnp.float32, least / len(pieces), high / len(pieces))
        loudness = loudness * jnp.repeat(jnp.exp(heights), shape[axis_at] // parts).reshape((-1,) + (1,) * (len(shape) - 1 - axis_at))
    return loudness


def bell_draw(rng, dims, deviation, reach, pieces=(), dtype=jnp.bfloat16):
    loudness = steps_of(rng, dims, pieces, -0.22, 0.18) if pieces else 1.0
    result = jax.random.normal(rng, dims, jnp.float32) * deviation * loudness
    return jnp.minimum(jnp.maximum(result, -reach), reach).astype(dtype)


def setup_inputs(seed: int = 0) -> dict:
    streams_of = jax.random.split(jax.random.key(seed), 9)
    return {
        "tokens": draw_tokens(jax.random.fold_in(streams_of[8], 71), 0),
        "in_gain": jnp.clip(1.0 + 0.18 * jax.random.normal(streams_of[1], (D,), jnp.float32), 0.1, 1.9),
        "w_key": bell_draw(streams_of[2], (D, KVH * HD), D ** -0.5, 0.125, ((0, 32),)),
        "w_value": bell_draw(streams_of[3], (D, KVH * HD), D ** -0.5, 0.125, ((0, 32),)),
        "k_gain": jnp.clip(1.0 + 0.18 * jax.random.normal(streams_of[4], (HD,), jnp.float32), 0.1, 1.9),
        "new_query": bell_draw(streams_of[5], (SEQS, HEADS * HD), 1.0, 6.0),
        "q_gain": jnp.clip(1.0 + 0.18 * jax.random.normal(streams_of[6], (HD,), jnp.float32), 0.1, 1.9),
        "stick_bias": draw_stick_bias(jax.random.fold_in(streams_of[8], 71), 0),
    }


NORM_EPS = 1e-06

def root_norm(values, scaling):
    inverse = lax.rsqrt(lax.optimization_barrier(jnp.mean(values * values, axis=-1, keepdims=True)) + NORM_EPS)
    return values * inverse * scaling

def reference(tokens, in_gain, w_key, w_value, k_gain, new_query, q_gain, stick_bias):
    per_group = HEADS // KVH
    query_rows = root_norm(new_query.astype(jnp.float32).reshape(SEQS, KVH, per_group, HD), q_gain).astype(jnp.bfloat16)
    bias_rows = stick_bias.astype(jnp.float32).reshape(KVH, per_group)

    def per_sequence(inputs):
        seq_tokens, seq_query = inputs
        normed = root_norm(seq_tokens.astype(jnp.float32), in_gain).astype(jnp.bfloat16)
        key_raw = jnp.dot(normed, w_key, preferred_element_type=jnp.float32).reshape(LENGTH, KVH, HD)
        key_rows = root_norm(key_raw, k_gain).astype(jnp.bfloat16)
        value_rows = jnp.dot(normed, w_value, preferred_element_type=jnp.float32).astype(jnp.bfloat16).reshape(LENGTH, KVH, HD)
        scores = jnp.einsum('hqe,phe->hqp', seq_query.astype(jnp.float32), key_rows.astype(jnp.float32)) * HD ** (-0.5) + bias_rows[:, :, None]
        log_keep = jax.nn.log_sigmoid(-scores)
        log_after = lax.cumsum(log_keep, axis=2, reverse=True) - log_keep
        weights = jnp.exp(jax.nn.log_sigmoid(scores) + log_after).astype(jnp.bfloat16)
        read_rows = jnp.einsum('hqp,phe->hqe', weights.astype(jnp.float32), value_rows.astype(jnp.float32))
        return (key_rows.transpose(1, 0, 2), value_rows.transpose(1, 0, 2), read_rows.reshape(KVH, per_group * HD))
    key_all, value_all, read_all = lax.map(per_sequence, (tokens, query_rows))
    key_cache = key_all.transpose(1, 0, 2, 3).reshape(KVH * SEQS, LENGTH, HD)
    value_cache = value_all.transpose(1, 0, 2, 3).reshape(KVH * SEQS, LENGTH, HD)
    read_out = read_all.transpose(1, 0, 2).reshape(KVH * SEQS, per_group * HD)
    return (key_cache, value_cache, read_out)
```

```python
import functools

import jax
import jax.numpy as jnp
from jax import lax
from jax.experimental import pallas as pl
from jax.experimental.pallas import tpu as pltpu
from jax.sharding import PartitionSpec as P

MESH = pl.DeviceIdType.MESH
NORM_EPS = 1e-06
F32 = jnp.float32
BF16 = jnp.bfloat16

Z = 16
SIDE = 4
SEQS = 8
TOK = 96
PAIR = 2 * TOK
D = 2048
HD = 128
SPAN = Z * PAIR
CHUNKS = SPAN // HD


def log1p_unit(e):
    t = e / (2.0 + e)
    t2 = t * t
    acc = jnp.full_like(t, 1.0 / 15.0)
    for n in (13.0, 11.0, 9.0, 7.0, 5.0, 3.0):
        acc = acc * t2 + 1.0 / n
    return 2.0 * t * (acc * t2 + 1.0)


def far_first(i):
    return Z // 2 + (1 - 2 * (i % 2)) * ((i + 1) // 2)


def kernel(
    tokens_ref, in_gain_ref, w_key_ref, w_value_ref, k_gain_ref, query_ref, q_gain_ref, bias_ref,
    key_out, value_out, read_out,
    raw, normed, weights, sendbuf, kv, scores, queries, qflat, parts,
    tok_sem, wz_send, wz_recv, wl_sem, w1_send, w1_recv, w2_send, w2_recv, x_send, x_recv,
    kv_send, kv_recv, out_sem, p_send, p_recv,
):
    sp = lax.axis_index("sp")
    tp = lax.axis_index("tp")
    z, core = tp // 2, tp % 2
    y, x = sp // SIDE, sp % SIDE
    first, second = y + core * (x - y), x + core * (y - x)
    first_step, second_step = SIDE - 3 * core, 1 + 3 * core

    barrier = pltpu.get_barrier_semaphore()

    def greet_tp(i, carry):
        pl.semaphore_signal(barrier, inc=1, device_id=(sp, (tp + i) % (2 * Z)), device_id_type=MESH)
        return carry

    def greet_sp(i, carry):
        pl.semaphore_signal(barrier, inc=1, device_id=((sp + i) % (SIDE * SIDE), tp), device_id_type=MESH)
        return carry

    lax.fori_loop(1, 2 * Z, greet_tp, 0)
    lax.fori_loop(1, SIDE * SIDE, greet_sp, 0)

    def fetch(s, carry):
        pltpu.make_async_copy(tokens_ref.at[s], raw.at[s], tok_sem.at[s]).start()
        return carry

    lax.fori_loop(0, SEQS, fetch, 0)

    for i in range(8):
        qflat[i] = query_ref[:, pl.ds(i * HD, HD)].astype(F32)
    group, seq = tp // SEQS, tp % SEQS
    queries[...] = jnp.zeros_like(queries)
    for i in range(2):
        head = qflat[group * 2 + i, pl.ds(seq, 1), :]
        inverse = lax.rsqrt(jnp.mean(head * head, axis=-1, keepdims=True) + NORM_EPS)
        queries[pl.ds(i, 1), :] = head * inverse * q_gain_ref[...]

    pl.semaphore_wait(barrier, 2 * Z - 1 + SIDE * SIDE - 1)

    def tile_of(target_core, to_z):
        ref = (w_key_ref, w_value_ref)[target_core]
        rows, cols = ((y, x), (x, y))[target_core]
        return ref.at[pl.ds(pl.multiple_of(rows * 16, 16), 16), pl.ds(pl.multiple_of((cols + to_z) % SIDE * HD, HD), HD)]

    def landing(target_core):
        return weights.at[0, tp, (y, x)[target_core]]

    def deal(i, carry):
        to_z = (z + far_first(i)) % Z
        for target_core in range(2):
            pltpu.make_async_remote_copy(
                tile_of(target_core, to_z), landing(target_core), wz_send, wz_recv,
                device_id=(sp, to_z * 2 + target_core), device_id_type=MESH,
            ).start()
        return carry

    lax.fori_loop(0, Z - 1, deal, 0)
    for target_core in range(2):
        @pl.when(core == target_core)
        def _():
            pltpu.make_async_copy(tile_of(target_core, z), landing(target_core), wl_sem).start()

        @pl.when(core != target_core)
        def _():
            pltpu.make_async_remote_copy(
                tile_of(target_core, z), landing(target_core), wz_send, wz_recv,
                device_id=(sp, z * 2 + target_core), device_id_type=MESH,
            ).start()

    def norm(s, carry):
        pltpu.make_async_copy(tokens_ref.at[s], raw.at[s], tok_sem.at[s]).wait()
        for part in range(TOK // 16):
            rows = raw[s, pl.ds(part * 16, 16), :].astype(F32)
            inverse = lax.rsqrt(jnp.mean(rows * rows, axis=-1, keepdims=True) + NORM_EPS)
            normed[s, core, pl.ds(part * 16, 16), :] = (rows * inverse * in_gain_ref[...]).astype(BF16)
        pltpu.make_async_remote_copy(
            normed.at[s, core], normed.at[s, core], x_send, x_recv,
            device_id=(sp, z * 2 + 1 - core), device_id_type=MESH,
        ).start()
        return carry

    lax.fori_loop(0, SEQS, norm, 0)

    def sp_of(a, b):
        return a * first_step + b * second_step

    pltpu.make_async_copy(landing(0), landing(0), wl_sem).wait()
    column = weights.at[0, pl.ds(0, 2 * Z - 1), 0]
    pltpu.make_async_copy(column, column, wz_recv).wait()
    strip = weights.at[0, :, first]
    for i in (1, 3, 2):
        pltpu.make_async_remote_copy(
            strip, strip, w1_send, w1_recv,
            device_id=(sp_of((first + i) % SIDE, second), tp), device_id_type=MESH,
        ).start()
    three = weights.at[0, :, pl.ds(0, 3)]
    pltpu.make_async_copy(three, three, w1_recv).wait()
    for i in (1, 3, 2):
        pltpu.make_async_remote_copy(
            weights.at[0], weights.at[i], w2_send, w2_recv.at[i],
            device_id=(sp_of(first, (second + SIDE - i) % SIDE), tp), device_id_type=MESH,
        ).start()

    half = normed.at[:, 0]
    pltpu.make_async_copy(half, half, x_recv).wait()

    for slot in (0, 1, 3, 2):
        if slot:
            pltpu.make_async_copy(weights.at[slot], weights.at[slot], w2_recv.at[slot]).wait()
        head = (second + slot + z) % SIDE

        def project(s, carry):
            raw_rows = jnp.dot(
                normed[s].reshape(PAIR, D), weights[slot].reshape(D, HD), preferred_element_type=F32
            )
            inverse = lax.rsqrt(jnp.mean(raw_rows * raw_rows, axis=-1, keepdims=True) + NORM_EPS)
            out = jnp.where(core == 0, raw_rows * inverse * k_gain_ref[...], raw_rows)
            sendbuf[slot * SEQS + s] = out.astype(BF16)
            target = head * SEQS + s
            source = sendbuf.at[slot * SEQS + s]
            there = kv.at[core, pl.ds(pl.multiple_of(z * PAIR, PAIR), PAIR)]

            @pl.when(target == tp)
            def _():
                pltpu.make_async_copy(source, there, kv_recv.at[core, z]).start()

            @pl.when(target != tp)
            def _():
                pltpu.make_async_remote_copy(
                    source, there, kv_send, kv_recv.at[core, z],
                    device_id=(sp, target), device_id_type=MESH,
                ).start()

            return carry

        lax.fori_loop(0, SEQS, project, 0)

    query = queries[...].astype(BF16)

    def score(pair, carry):
        for i in range(2):
            at = pair * 2 + i
            block = kv.at[0, pl.ds(pl.multiple_of(at * PAIR, PAIR), PAIR)]
            pltpu.make_async_copy(block, block, kv_recv.at[0, at]).wait()
        for i in range(3):
            chunk = pair * 3 + i
            keys = kv[0, pl.ds(pl.multiple_of(chunk * HD, HD), HD), :]
            scores[chunk] = lax.dot_general(query, keys, (((1,), (1,)), ((), ())), preferred_element_type=F32)[:8]
        span = pl.ds(pl.multiple_of(pair * 2 * PAIR, 2 * PAIR), 2 * PAIR)
        pltpu.make_async_copy(kv.at[0, span], key_out.at[0, span], out_sem).start()
        return carry

    lax.fori_loop(0, Z // 2, score, 0)

    row = lax.broadcasted_iota(jnp.int32, (1, 8, HD), 1)
    bias = jnp.where(row == 0, bias_ref[group * 2], bias_ref[group * 2 + 1])
    score_all = scores[...] * (HD ** -0.5) + bias
    soft = log1p_unit(jnp.exp(-jnp.abs(score_all)))
    log_keep = -(jnp.maximum(score_all, 0.0) + soft)
    log_take = -(jnp.maximum(-score_all, 0.0) + soft)
    later = (
        lax.broadcasted_iota(jnp.int32, (HD, HD), 0) > lax.broadcasted_iota(jnp.int32, (HD, HD), 1)
    ).astype(F32)
    after = jnp.dot(
        log_keep.reshape(CHUNKS * 8, HD), later, preferred_element_type=F32, precision=lax.Precision.HIGHEST
    ).reshape(CHUNKS, 8, HD)
    totals = jnp.sum(log_keep, axis=2, keepdims=True)
    carried = jnp.zeros((8, 1), F32)
    chunk_weights = [None] * CHUNKS
    for chunk in reversed(range(CHUNKS)):
        chunk_weights[chunk] = jnp.exp(log_take[chunk] + after[chunk] + carried).astype(BF16)
        carried = carried + totals[chunk]

    def arrive(at, carry):
        block = kv.at[1, pl.ds(pl.multiple_of(at * PAIR, PAIR), PAIR)]
        pltpu.make_async_copy(block, block, kv_recv.at[1, at]).wait()
        return carry

    lax.fori_loop(0, Z, arrive, 0)
    pltpu.make_async_copy(kv.at[1], value_out.at[0], out_sem).start()
    partial = jnp.zeros((8, HD), F32)
    for chunk in range(CHUNKS):
        partial = partial + jnp.dot(
            chunk_weights[chunk], kv[1, pl.ds(chunk * HD, HD), :], preferred_element_type=F32
        )

    parts[sp, pl.ds(0, 8), :] = partial
    parts[sp, pl.ds(8, 8), :] = jnp.broadcast_to(carried, (8, HD))

    def share(i, carry):
        pltpu.make_async_remote_copy(
            parts.at[sp], parts.at[sp], p_send, p_recv,
            device_id=((sp + i) % (SIDE * SIDE), tp), device_id_type=MESH,
        ).start()
        return carry

    lax.fori_loop(1, SIDE * SIDE, share, 0)
    others = parts.at[pl.ds(0, SIDE * SIDE - 1)]
    pltpu.make_async_copy(others, others, p_recv).wait()
    total = jnp.zeros((8, HD), F32)
    log_later = jnp.zeros((8, HD), F32)
    for span in reversed(range(SIDE * SIDE)):
        total = total + jnp.exp(log_later) * parts[span, pl.ds(0, 8), :]
        log_later = log_later + parts[span, pl.ds(8, 8), :]
    read_out[:, pl.ds(0, HD)] = total[0:1]
    read_out[:, pl.ds(HD, HD)] = total[1:2]

    pltpu.make_async_copy(column, column, wz_send).wait()
    pltpu.make_async_copy(three, three, w1_send).wait()
    pltpu.make_async_copy(weights.at[pl.ds(0, 3)], weights.at[pl.ds(0, 3)], w2_send).wait()
    pltpu.make_async_copy(half, half, x_send).wait()

    sent = sendbuf.at[pl.ds(0, 2 * Z - 1)]
    pltpu.make_async_copy(sent, sent, kv_send).wait()
    pltpu.make_async_copy(others, others, p_send).wait()
    pltpu.make_async_copy(kv.at[0], key_out.at[0], out_sem).wait()
    pltpu.make_async_copy(kv.at[1], value_out.at[0], out_sem).wait()


def shards(tokens, in_gain, w_key, w_value, k_gain, new_query, q_gain, stick_bias):
    vmem = pl.BlockSpec(memory_space=pltpu.VMEM)
    hbm = pl.BlockSpec(memory_space=pl.ANY)
    dma = pltpu.SemaphoreType.DMA
    return pl.pallas_call(
        kernel,
        out_shape=(
            jax.ShapeDtypeStruct((1, SPAN, HD), BF16),
            jax.ShapeDtypeStruct((1, SPAN, HD), BF16),
            jax.ShapeDtypeStruct((1, 2 * HD), F32),
        ),
        in_specs=[hbm, vmem, vmem, vmem, vmem, vmem, vmem, pl.BlockSpec(memory_space=pltpu.SMEM)],
        out_specs=(hbm, hbm, vmem),
        scratch_shapes=[
            pltpu.VMEM((SEQS, TOK, D), BF16),
            pltpu.VMEM((SEQS, 2, TOK, D), BF16),
            pltpu.VMEM((SIDE, 2 * Z, 4, 16, HD), BF16),
            pltpu.VMEM((2 * Z, PAIR, HD), BF16),
            pltpu.VMEM((2, SPAN, HD), BF16),
            pltpu.VMEM((CHUNKS, 8, HD), F32),
            pltpu.VMEM((16, HD), F32),
            pltpu.VMEM((8, SEQS, HD), F32),
            pltpu.VMEM((SIDE * SIDE, 16, HD), F32),
            dma((SEQS,)), dma, dma, dma, dma, dma, dma, dma((SIDE,)), dma, dma,
            dma, dma((2, Z)), dma, dma, dma,
        ],
        compiler_params=pltpu.CompilerParams(
            collective_id=0, has_side_effects=True, vmem_limit_bytes=40 * 2**20
        ),
    )(
        tokens, in_gain.reshape(1, D), w_key, w_value, k_gain.reshape(1, HD), new_query,
        q_gain.reshape(1, HD), stick_bias,
    )


def solution(mesh):
    return jax.shard_map(
        shards,
        mesh=mesh,
        in_specs=(
            P(None, ("sp", "tp"), None), P(), P("tp", None), P("tp", None), P(), P(), P(), P(),
        ),
        out_specs=(P("tp", "sp", None), P("tp", "sp", None), P("tp", None)),
        check_vma=False,
    )
```

```python
import functools

import jax
import jax.numpy as jnp
from jax import lax
from jax.experimental import pallas as pl
from jax.experimental.pallas import tpu as pltpu
from jax.sharding import PartitionSpec as P

MESH = pl.DeviceIdType.MESH
NORM_EPS = 1e-06
F32 = jnp.float32
BF16 = jnp.bfloat16

Z = 16
SIDE = 4
SEQS = 8
TOK = 96
PAIR = 2 * TOK
D = 2048
HD = 128
SPAN = Z * PAIR
CHUNKS = SPAN // HD


def log1p_unit(e):
    t = e / (2.0 + e)
    t2 = t * t
    acc = jnp.full_like(t, 1.0 / 15.0)
    for n in (13.0, 11.0, 9.0, 7.0, 5.0, 3.0):
        acc = acc * t2 + 1.0 / n
    return 2.0 * t * (acc * t2 + 1.0)


def far_first(i):
    return Z // 2 + (1 - 2 * (i % 2)) * ((i + 1) // 2)


def kernel(
    tokens_ref, in_gain_in, w_key_in, w_value_in, k_gain_in, query_in, q_gain_in, bias_in,
    key_out, value_out, read_out,
    in_gain_ref, w_key_ref, w_value_ref, k_gain_ref, query_ref, q_gain_ref, bias_ref,
    raw, normed, weights, sendbuf, scores, queries, qflat, parts,
    in_sem, tok_sem, wz_send, wz_recv, wl_sem, w1_send, w1_recv, w2_send, w2_recv, x_send, x_recv,
    kv_send, kv_recv, p_send, p_recv,
):
    sp = lax.axis_index("sp")
    tp = lax.axis_index("tp")
    z, core = tp // 2, tp % 2
    y, x = sp // SIDE, sp % SIDE
    first, second = y + core * (x - y), x + core * (y - x)
    first_step, second_step = SIDE - 3 * core, 1 + 3 * core

    barrier = pltpu.get_barrier_semaphore()

    def greet_tp(i, carry):
        pl.semaphore_signal(barrier, inc=1, device_id=(sp, (tp + i) % (2 * Z)), device_id_type=MESH)
        return carry

    def greet_sp(i, carry):
        pl.semaphore_signal(barrier, inc=1, device_id=((sp + i) % (SIDE * SIDE), tp), device_id_type=MESH)
        return carry

    lax.fori_loop(1, 2 * Z, greet_tp, 0)
    lax.fori_loop(1, SIDE * SIDE, greet_sp, 0)

    fetched = [
        pltpu.make_async_copy(source, target, in_sem.at[i])
        for i, (source, target) in enumerate((
            (w_key_in, w_key_ref), (w_value_in, w_value_ref), (query_in, query_ref), (q_gain_in, q_gain_ref),
            (in_gain_in, in_gain_ref), (k_gain_in, k_gain_ref), (bias_in, bias_ref),
        ))
    ]
    for copy in fetched:
        copy.start()

    def fetch(s, carry):
        pltpu.make_async_copy(tokens_ref.at[s], raw.at[s], tok_sem.at[s]).start()
        return carry

    lax.fori_loop(0, SEQS, fetch, 0)

    for copy in fetched:
        copy.wait()

    for i in range(8):
        qflat[i] = query_ref[:, pl.ds(i * HD, HD)].astype(F32)
    group, seq = tp // SEQS, tp % SEQS
    queries[...] = jnp.zeros_like(queries)
    for i in range(2):
        head = qflat[group * 2 + i, pl.ds(seq, 1), :]
        inverse = lax.rsqrt(jnp.mean(head * head, axis=-1, keepdims=True) + NORM_EPS)
        queries[pl.ds(i, 1), :] = head * inverse * q_gain_ref[...]

    with jax.named_scope("barrier"):
        pl.semaphore_wait(barrier, 2 * Z - 1 + SIDE * SIDE - 1)

    def tile_of(target_core, to_z):
        ref = (w_key_ref, w_value_ref)[target_core]
        rows, cols = ((y, x), (x, y))[target_core]
        return ref.at[pl.ds(pl.multiple_of(rows * 16, 16), 16), pl.ds(pl.multiple_of((cols + to_z) % SIDE * HD, HD), HD)]

    def landing(target_core):
        return weights.at[0, tp, (y, x)[target_core]]

    def deal(i, carry):
        to_z = (z + far_first(i)) % Z
        for target_core in range(2):
            pltpu.make_async_remote_copy(
                tile_of(target_core, to_z), landing(target_core), wz_send, wz_recv,
                device_id=(sp, to_z * 2 + target_core), device_id_type=MESH,
            ).start()
        return carry

    with jax.named_scope("deal"):
        lax.fori_loop(0, Z - 1, deal, 0)
    for target_core in range(2):
        @pl.when(core == target_core)
        def _():
            pltpu.make_async_copy(tile_of(target_core, z), landing(target_core), wl_sem).start()

        @pl.when(core != target_core)
        def _():
            pltpu.make_async_remote_copy(
                tile_of(target_core, z), landing(target_core), wz_send, wz_recv,
                device_id=(sp, z * 2 + target_core), device_id_type=MESH,
            ).start()

    def norm(s, carry):
        pltpu.make_async_copy(tokens_ref.at[s], raw.at[s], tok_sem.at[s]).wait()
        for part in range(TOK // 16):
            rows = raw[s, pl.ds(part * 16, 16), :].astype(F32)
            inverse = lax.rsqrt(jnp.mean(rows * rows, axis=-1, keepdims=True) + NORM_EPS)
            normed[s, core, pl.ds(part * 16, 16), :] = (rows * inverse * in_gain_ref[...]).astype(BF16)
        pltpu.make_async_remote_copy(
            normed.at[s, core], normed.at[s, core], x_send, x_recv,
            device_id=(sp, z * 2 + 1 - core), device_id_type=MESH,
        ).start()
        return carry

    with jax.named_scope("norm"):
        lax.fori_loop(0, SEQS, norm, 0)

    def sp_of(a, b):
        return a * first_step + b * second_step

    pltpu.make_async_copy(landing(0), landing(0), wl_sem).wait()
    column = weights.at[0, pl.ds(0, 2 * Z - 1), 0]
    with jax.named_scope("z_phase"):
        pltpu.make_async_copy(column, column, wz_recv).wait()
    strip = weights.at[0, :, first]
    for i in (1, 3, 2):
        pltpu.make_async_remote_copy(
            strip, strip, w1_send, w1_recv,
            device_id=(sp_of((first + i) % SIDE, second), tp), device_id_type=MESH,
        ).start()
    three = weights.at[0, :, pl.ds(0, 3)]
    with jax.named_scope("first_phase"):
        pltpu.make_async_copy(three, three, w1_recv).wait()
    for i in (1, 3, 2):
        pltpu.make_async_remote_copy(
            weights.at[0], weights.at[i], w2_send, w2_recv.at[i],
            device_id=(sp_of(first, (second + SIDE - i) % SIDE), tp), device_id_type=MESH,
        ).start()

    half = normed.at[:, 0]
    with jax.named_scope("partner"):
        pltpu.make_async_copy(half, half, x_recv).wait()

    for slot in (0, 1, 3, 2):
        if slot:
            with jax.named_scope("slot"):
                pltpu.make_async_copy(weights.at[slot], weights.at[slot], w2_recv.at[slot]).wait()
        head = (second + slot + z) % SIDE

        def project(s, carry):
            raw_rows = jnp.dot(
                normed[s].reshape(PAIR, D), weights[slot].reshape(D, HD), preferred_element_type=F32
            )
            inverse = lax.rsqrt(jnp.mean(raw_rows * raw_rows, axis=-1, keepdims=True) + NORM_EPS)
            out = jnp.where(core == 0, raw_rows * inverse * k_gain_ref[...], raw_rows)
            sendbuf[slot * SEQS + s] = out.astype(BF16)
            target = head * SEQS + s
            source = sendbuf.at[slot * SEQS + s]
            for which, out_ref in enumerate((key_out, value_out)):
                there = out_ref.at[0, pl.ds(pl.multiple_of(z * PAIR, PAIR), PAIR)]

                @pl.when(jnp.logical_and(core == which, target == tp))
                def _():
                    pltpu.make_async_copy(source, there, kv_recv.at[which, z]).start()

                @pl.when(jnp.logical_and(core == which, target != tp))
                def _():
                    pltpu.make_async_remote_copy(
                        source, there, kv_send, kv_recv.at[which, z],
                        device_id=(sp, target), device_id_type=MESH,
                    ).start()

            return carry

        with jax.named_scope("project"):
            lax.fori_loop(0, SEQS, project, 0)

    query = queries[...].astype(BF16)

    def score(pair, carry):
        for i in range(2):
            at = pair * 2 + i
            block = key_out.at[0, pl.ds(pl.multiple_of(at * PAIR, PAIR), PAIR)]
            pltpu.make_async_copy(block, block, kv_recv.at[0, at]).wait()
        for i in range(3):
            chunk = pair * 3 + i
            keys = key_out[0, pl.ds(pl.multiple_of(chunk * HD, HD), HD), :]
            scores[chunk] = lax.dot_general(query, keys, (((1,), (1,)), ((), ())), preferred_element_type=F32)[:8]
        return carry

    with jax.named_scope("score"):
        lax.fori_loop(0, Z // 2, score, 0)

    row = lax.broadcasted_iota(jnp.int32, (1, 8, HD), 1)
    bias = jnp.where(row == 0, bias_ref[group * 2], bias_ref[group * 2 + 1])
    score_all = scores[...] * (HD ** -0.5) + bias
    soft = log1p_unit(jnp.exp(-jnp.abs(score_all)))
    log_keep = -(jnp.maximum(score_all, 0.0) + soft)
    log_take = -(jnp.maximum(-score_all, 0.0) + soft)
    later = (
        lax.broadcasted_iota(jnp.int32, (HD, HD), 0) > lax.broadcasted_iota(jnp.int32, (HD, HD), 1)
    ).astype(F32)
    after = jnp.dot(
        log_keep.reshape(CHUNKS * 8, HD), later, preferred_element_type=F32, precision=lax.Precision.HIGHEST
    ).reshape(CHUNKS, 8, HD)
    totals = jnp.sum(log_keep, axis=2, keepdims=True)
    carried = jnp.zeros((8, 1), F32)
    chunk_weights = [None] * CHUNKS
    for chunk in reversed(range(CHUNKS)):
        chunk_weights[chunk] = jnp.exp(log_take[chunk] + after[chunk] + carried).astype(BF16)
        carried = carried + totals[chunk]

    def arrive(at, carry):
        block = value_out.at[0, pl.ds(pl.multiple_of(at * PAIR, PAIR), PAIR)]
        pltpu.make_async_copy(block, block, kv_recv.at[1, at]).wait()
        return carry

    with jax.named_scope("arrive"):
        lax.fori_loop(0, Z, arrive, 0)
    partial = jnp.zeros((8, HD), F32)
    for chunk in range(CHUNKS):
        partial = partial + jnp.dot(
            chunk_weights[chunk], value_out[0, pl.ds(chunk * HD, HD), :], preferred_element_type=F32
        )

    parts[sp, pl.ds(0, 8), :] = partial
    parts[sp, pl.ds(8, 8), :] = jnp.broadcast_to(carried, (8, HD))

    def share(i, carry):
        pltpu.make_async_remote_copy(
            parts.at[sp], parts.at[sp], p_send, p_recv,
            device_id=((sp + i) % (SIDE * SIDE), tp), device_id_type=MESH,
        ).start()
        return carry

    lax.fori_loop(1, SIDE * SIDE, share, 0)
    others = parts.at[pl.ds(0, SIDE * SIDE - 1)]
    with jax.named_scope("others"):
        pltpu.make_async_copy(others, others, p_recv).wait()
    total = jnp.zeros((8, HD), F32)
    log_later = jnp.zeros((8, HD), F32)
    for span in reversed(range(SIDE * SIDE)):
        total = total + jnp.exp(log_later) * parts[span, pl.ds(0, 8), :]
        log_later = log_later + parts[span, pl.ds(8, 8), :]
    read_out[:, pl.ds(0, HD)] = total[0:1]
    read_out[:, pl.ds(HD, HD)] = total[1:2]

    pltpu.make_async_copy(column, column, wz_send).wait()
    pltpu.make_async_copy(three, three, w1_send).wait()
    pltpu.make_async_copy(weights.at[pl.ds(0, 3)], weights.at[pl.ds(0, 3)], w2_send).wait()
    pltpu.make_async_copy(half, half, x_send).wait()

    sent = sendbuf.at[pl.ds(0, 2 * Z - 1)]
    with jax.named_scope("drain"):
        pltpu.make_async_copy(sent, sent, kv_send).wait()
    pltpu.make_async_copy(others, others, p_send).wait()


def shards(tokens, in_gain, w_key, w_value, k_gain, new_query, q_gain, stick_bias):
    vmem = pl.BlockSpec(memory_space=pltpu.VMEM)
    hbm = pl.BlockSpec(memory_space=pltpu.HBM)
    dma = pltpu.SemaphoreType.DMA
    return pl.pallas_call(
        kernel,
        out_shape=(
            jax.ShapeDtypeStruct((1, SPAN, HD), BF16),
            jax.ShapeDtypeStruct((1, SPAN, HD), BF16),
            jax.ShapeDtypeStruct((1, 2 * HD), F32),
        ),
        in_specs=[hbm] * 8,
        out_specs=(vmem, vmem, vmem),
        scratch_shapes=[
            pltpu.VMEM((1, D), F32),
            pltpu.VMEM(w_key.shape, BF16),
            pltpu.VMEM(w_value.shape, BF16),
            pltpu.VMEM((1, HD), F32),
            pltpu.VMEM(new_query.shape, BF16),
            pltpu.VMEM((1, HD), F32),
            pltpu.SMEM(stick_bias.shape, F32),
            pltpu.VMEM((SEQS, TOK, D), BF16),
            pltpu.VMEM((SEQS, 2, TOK, D), BF16),
            pltpu.VMEM((SIDE, 2 * Z, 4, 16, HD), BF16),
            pltpu.VMEM((2 * Z, PAIR, HD), BF16),
            pltpu.VMEM((CHUNKS, 8, HD), F32),
            pltpu.VMEM((16, HD), F32),
            pltpu.VMEM((8, SEQS, HD), F32),
            pltpu.VMEM((SIDE * SIDE, 16, HD), F32),
            dma((7,)), dma((SEQS,)), dma, dma, dma, dma, dma, dma, dma((SIDE,)), dma, dma,
            dma, dma((2, Z)), dma, dma,
        ],
        compiler_params=pltpu.CompilerParams(
            collective_id=0, has_side_effects=True, vmem_limit_bytes=40 * 2**20
        ),
    )(
        *(
            pltpu.with_memory_space_constraint(a, pltpu.HBM)
            for a in (
                tokens, in_gain.reshape(1, D), w_key, w_value, k_gain.reshape(1, HD), new_query,
                q_gain.reshape(1, HD), stick_bias,
            )
        )
    )


def solution(mesh):
    return jax.shard_map(
        shards,
        mesh=mesh,
        in_specs=(
            P(None, ("sp", "tp"), None), P(), P("tp", None), P("tp", None), P(), P(), P(), P(),
        ),
        out_specs=(P("tp", "sp", None), P("tp", "sp", None), P("tp", None)),
        check_vma=False,
    )
```

```python
import functools

import jax
import jax.numpy as jnp
from jax import lax
from jax.experimental import pallas as pl
from jax.experimental.pallas import tpu as pltpu
from jax.sharding import PartitionSpec as P

MESH = pl.DeviceIdType.MESH
NORM_EPS = 1e-06
F32 = jnp.float32
BF16 = jnp.bfloat16

Z = 16
SIDE = 4
SEQS = 8
TOK = 96
PAIR = 2 * TOK
D = 2048
HD = 128
SPAN = Z * PAIR
CHUNKS = SPAN // HD


def log1p_unit(e):
    t = e / (2.0 + e)
    t2 = t * t
    acc = jnp.full_like(t, 1.0 / 15.0)
    for n in (13.0, 11.0, 9.0, 7.0, 5.0, 3.0):
        acc = acc * t2 + 1.0 / n
    return 2.0 * t * (acc * t2 + 1.0)


def turn(target_core, chip_z):
    return chip_z // SIDE + (chip_z + target_core * (Z - 2 * chip_z))


def half_of(slot):
    return 0 if slot == 1 else Z


def far_first(i):
    return Z // 2 + (1 - 2 * (i % 2)) * ((i + 1) // 2)


def kernel(
    tokens_ref, in_gain_in, w_key_in, w_value_in, k_gain_in, query_in, q_gain_in, bias_in,
    key_out, value_out, parts,
    in_gain_ref, w_key_ref, w_value_ref, k_gain_ref, query_ref, q_gain_ref, bias_ref,
    raw, normed, weights, sendbuf, scores, queries, qflat,
    in_sem, tok_sem, wz_send, wz_recv, wl_sem, w1_send, w1_recv, w2_send, w2_recv, x_send, x_recv,
    kv_send, kv_recv, p_send, p_recv,
):
    sp = lax.axis_index("sp")
    tp = lax.axis_index("tp")
    z, core = tp // 2, tp % 2
    y, x = sp // SIDE, sp % SIDE
    first, second = y + core * (x - y), x + core * (y - x)
    first_step, second_step = SIDE - 3 * core, 1 + 3 * core

    barrier = pltpu.get_barrier_semaphore()

    def greet_tp(i, carry):
        pl.semaphore_signal(barrier, inc=1, device_id=(sp, (tp + i) % (2 * Z)), device_id_type=MESH)
        return carry

    def greet_sp(i, carry):
        pl.semaphore_signal(barrier, inc=1, device_id=((sp + i) % (SIDE * SIDE), tp), device_id_type=MESH)
        return carry

    lax.fori_loop(1, 2 * Z, greet_tp, 0)
    lax.fori_loop(1, SIDE * SIDE, greet_sp, 0)

    fetched = [
        pltpu.make_async_copy(source, target, in_sem.at[i])
        for i, (source, target) in enumerate((
            (w_key_in, w_key_ref), (w_value_in, w_value_ref), (query_in, query_ref), (q_gain_in, q_gain_ref),
            (in_gain_in, in_gain_ref), (k_gain_in, k_gain_ref), (bias_in, bias_ref),
        ))
    ]
    for copy in fetched:
        copy.start()

    def fetch(s, carry):
        pltpu.make_async_copy(tokens_ref.at[s], raw.at[s], tok_sem.at[s]).start()
        return carry

    lax.fori_loop(0, SEQS, fetch, 0)

    for copy in fetched:
        copy.wait()

    for i in range(8):
        qflat[i] = query_ref[:, pl.ds(i * HD, HD)].astype(F32)
    group, seq = tp // SEQS, tp % SEQS
    queries[...] = jnp.zeros_like(queries)
    for i in range(2):
        head = qflat[group * 2 + i, pl.ds(seq, 1), :]
        inverse = lax.rsqrt(jnp.mean(head * head, axis=-1, keepdims=True) + NORM_EPS)
        head = head * inverse * q_gain_ref[...]
        queries[pl.ds(i, 1), :] = head
        queries[pl.ds(i + 2, 1), :] = head

    with jax.named_scope("barrier"):
        pl.semaphore_wait(barrier, 2 * Z - 1 + SIDE * SIDE - 1)

    def tile_of(target_core, to_z):
        ref = (w_key_ref, w_value_ref)[target_core]
        rows, cols = ((y, x), (x, y))[target_core]
        return ref.at[pl.ds(pl.multiple_of(rows * 16, 16), 16), pl.ds(pl.multiple_of((cols + turn(target_core, to_z)) % SIDE * HD, HD), HD)]

    def landing(target_core):
        return weights.at[0, tp, (y, x)[target_core]]

    def deal(i, carry):
        to_z = (z + far_first(i)) % Z
        for target_core in range(2):
            pltpu.make_async_remote_copy(
                tile_of(target_core, to_z), landing(target_core), wz_send, wz_recv.at[z],
                device_id=(sp, to_z * 2 + target_core), device_id_type=MESH,
            ).start()
        return carry

    with jax.named_scope("deal"):
        lax.fori_loop(0, Z - 1, deal, 0)
    for target_core in range(2):
        @pl.when(core == target_core)
        def _():
            pltpu.make_async_copy(tile_of(target_core, z), landing(target_core), wl_sem).start()

        @pl.when(core != target_core)
        def _():
            pltpu.make_async_remote_copy(
                tile_of(target_core, z), landing(target_core), wz_send, wz_recv.at[z],
                device_id=(sp, z * 2 + target_core), device_id_type=MESH,
            ).start()

    def norm(s, carry):
        pltpu.make_async_copy(tokens_ref.at[s], raw.at[s], tok_sem.at[s]).wait()
        for part in range(TOK // 16):
            rows = raw[s, pl.ds(part * 16, 16), :].astype(F32)
            inverse = lax.rsqrt(jnp.mean(rows * rows, axis=-1, keepdims=True) + NORM_EPS)
            normed[s, core, pl.ds(part * 16, 16), :] = (rows * inverse * in_gain_ref[...]).astype(BF16)
        pltpu.make_async_remote_copy(
            normed.at[s, core], normed.at[s, core], x_send, x_recv,
            device_id=(sp, z * 2 + 1 - core), device_id_type=MESH,
        ).start()
        return carry

    with jax.named_scope("norm"):
        lax.fori_loop(0, SEQS, norm, 0)

    def sp_of(a, b):
        return a * first_step + b * second_step

    def pass_on(from_z):
        tiles = weights.at[0, pl.ds(from_z * 2, 2), first]
        for i in (2, 1, 3):
            pltpu.make_async_remote_copy(
                tiles, tiles, w1_send, w1_recv,
                device_id=(sp_of((first + i) % SIDE, second), tp), device_id_type=MESH,
            ).start()

    one, two = weights.at[0, 0, 0], weights.at[0, pl.ds(0, 2), 0]

    def forward(i, carry):
        from_z = (z + far_first(i)) % Z
        pltpu.make_async_copy(two, two, wz_recv.at[from_z]).wait()
        pass_on(from_z)
        return carry

    with jax.named_scope("z_phase"):
        lax.fori_loop(0, Z - 1, forward, 0)
        pltpu.make_async_copy(one, one, wl_sem).wait()
        pltpu.make_async_copy(one, one, wz_recv.at[z]).wait()
        pass_on(z)
    three = weights.at[0, :, pl.ds(0, 3)]
    with jax.named_scope("first_phase"):
        pltpu.make_async_copy(three, three, w1_recv).wait()

    def hand(source, slot, from_slot):
        target = weights.at[slot, pl.ds(half_of(from_slot), Z)] if slot == 2 else weights.at[slot]
        pltpu.make_async_remote_copy(
            source, target, w2_send, w2_recv.at[slot],
            device_id=(sp_of(first, (second + SIDE + from_slot - slot) % SIDE), tp), device_id_type=MESH,
        ).start()

    for slot in (1, 3):
        hand(weights.at[0], slot, 0)

    half = normed.at[:, 0]
    with jax.named_scope("partner"):
        pltpu.make_async_copy(half, half, x_recv).wait()

    def project(slot, i):
        head = (second + slot + turn(core, z)) % SIDE
        around = (head + SIDE - z // SIDE) % SIDE
        odd, back = around % 2, around // 2
        chip = odd * ((1 - back) * (3 - i) + back * i) + (1 - odd) * (i % 2 * (3 - i // 2) + (1 - i % 2) * (i // 2))
        for half_at in range(2):
            s = chip * 2 + (core + half_at) % 2
            raw_rows = jnp.dot(
                normed[s].reshape(PAIR, D), weights[slot].reshape(D, HD), preferred_element_type=F32
            )
            inverse = lax.rsqrt(jnp.mean(raw_rows * raw_rows, axis=-1, keepdims=True) + NORM_EPS)
            out = jnp.where(core == 0, raw_rows * inverse * k_gain_ref[...], raw_rows)
            sendbuf[slot * SEQS + s] = out.astype(BF16)
            target = head * SEQS + s
            source = sendbuf.at[slot * SEQS + s]
            for which, out_ref in enumerate((key_out, value_out)):
                there = out_ref.at[0, pl.ds(pl.multiple_of(z * PAIR, PAIR), PAIR)]

                @pl.when(jnp.logical_and(core == which, target == tp))
                def _():
                    pltpu.make_async_copy(source, there, kv_recv.at[which, z]).start()

                @pl.when(jnp.logical_and(core == which, target != tp))
                def _():
                    pltpu.make_async_remote_copy(
                        source, there, kv_send, kv_recv.at[which, z],
                        device_id=(sp, target), device_id_type=MESH,
                    ).start()

    for slots in ((0,), (1, 3), (2,)):
        for slot in slots:
            if slot:
                with jax.named_scope("slot"):
                    pltpu.make_async_copy(weights.at[slot], weights.at[slot], w2_recv.at[slot]).wait()
            if slot % 2:
                hand(weights.at[slot, pl.ds(half_of(slot), Z)], 2, slot)

        def project_all(i, carry):
            for slot in slots:
                project(slot, i)
            return carry

        with jax.named_scope("project"):
            lax.fori_loop(0, SIDE, project_all, 0)

    query = queries[...].astype(BF16)

    def score(pair, carry):
        for i in range(2):
            at = pair * 2 + i
            block = key_out.at[0, pl.ds(pl.multiple_of(at * PAIR, PAIR), PAIR)]
            pltpu.make_async_copy(block, block, kv_recv.at[0, at]).wait()
        for i in range(3):
            chunk = pair * 3 + i
            keys = key_out[0, pl.ds(pl.multiple_of(chunk * HD, HD), HD), :]
            scores[chunk] = lax.dot_general(query, keys, (((1,), (1,)), ((), ())), preferred_element_type=F32)[:8]
        return carry

    with jax.named_scope("score"):
        lax.fori_loop(0, Z // 2, score, 0)

    row = lax.broadcasted_iota(jnp.int32, (1, 8, HD), 1)
    bias = jnp.where(row % 2 == 0, bias_ref[group * 2], bias_ref[group * 2 + 1])
    score_all = scores[...] * (HD ** -0.5) + bias
    soft = log1p_unit(jnp.exp(-jnp.abs(score_all)))
    log_keep = -(jnp.maximum(score_all, 0.0) + soft)
    log_take = -(jnp.maximum(-score_all, 0.0) + soft)
    later = (
        lax.broadcasted_iota(jnp.int32, (HD, HD), 0) > lax.broadcasted_iota(jnp.int32, (HD, HD), 1)
    ).astype(F32)
    after = jnp.dot(
        log_keep.reshape(CHUNKS * 8, HD), later, preferred_element_type=F32, precision=lax.Precision.HIGHEST
    ).reshape(CHUNKS, 8, HD)
    totals = jnp.sum(log_keep, axis=2, keepdims=True)
    carried = jnp.zeros((8, 1), F32)
    chunk_weights = [None] * CHUNKS
    for chunk in reversed(range(CHUNKS)):
        chunk_weights[chunk] = jnp.exp(log_take[chunk] + after[chunk] + carried).astype(BF16)
        carried = carried + totals[chunk]

    def arrive(at, carry):
        block = value_out.at[0, pl.ds(pl.multiple_of(at * PAIR, PAIR), PAIR)]
        pltpu.make_async_copy(block, block, kv_recv.at[1, at]).wait()
        return carry

    with jax.named_scope("arrive"):
        lax.fori_loop(0, Z, arrive, 0)
    partial = jnp.zeros((8, HD), F32)
    for chunk in range(CHUNKS):
        partial = partial + jnp.dot(
            chunk_weights[chunk], value_out[0, pl.ds(chunk * HD, HD), :], preferred_element_type=F32
        )

    parts[sp] = jnp.where(row[0] < 2, partial, carried)

    def share(i, carry):
        pltpu.make_async_remote_copy(
            parts.at[sp], parts.at[sp], p_send, p_recv,
            device_id=((sp + i) % (SIDE * SIDE), tp), device_id_type=MESH,
        ).start()
        return carry

    lax.fori_loop(1, SIDE * SIDE, share, 0)
    others = parts.at[pl.ds(0, SIDE * SIDE - 1)]
    with jax.named_scope("others"):
        pltpu.make_async_copy(others, others, p_recv).wait()
    column = weights.at[0, pl.ds(0, 2 * Z - 1), 0]
    pltpu.make_async_copy(column, column, wz_send).wait()
    pltpu.make_async_copy(three, three, w1_send).wait()
    pltpu.make_async_copy(weights.at[pl.ds(0, 3)], weights.at[pl.ds(0, 3)], w2_send).wait()
    pltpu.make_async_copy(half, half, x_send).wait()

    sent = sendbuf.at[pl.ds(0, 2 * Z - 1)]
    with jax.named_scope("drain"):
        pltpu.make_async_copy(sent, sent, kv_send).wait()
    pltpu.make_async_copy(others, others, p_send).wait()


def write_out(key_ref, value_ref, parts_ref, key_out, value_out, read_out, read, sems):
    copies = [
        pltpu.make_async_copy(ref.at[0, pl.ds(i * (SPAN // 4), SPAN // 4)], out.at[0, pl.ds(i * (SPAN // 4), SPAN // 4)], sems.at[n, i])
        for n, (ref, out) in enumerate(((key_ref, key_out), (value_ref, value_out)))
        for i in range(4)
    ]
    for copy in copies:
        copy.start()
    total = jnp.zeros((2, HD), F32)
    log_later = jnp.zeros((2, HD), F32)
    for span in reversed(range(SIDE * SIDE)):
        total = total + jnp.exp(log_later) * parts_ref[span, pl.ds(0, 2), :]
        log_later = log_later + parts_ref[span, pl.ds(2, 2), :]
    read[:, pl.ds(0, HD)] = total[0:1]
    read[:, pl.ds(HD, HD)] = total[1:2]
    last = pltpu.make_async_copy(read, read_out, sems.at[2, 0])
    last.start()
    for copy in copies:
        copy.wait()
    last.wait()


def shards(tokens, in_gain, w_key, w_value, k_gain, new_query, q_gain, stick_bias):
    vmem = pl.BlockSpec(memory_space=pltpu.VMEM)
    hbm = pl.BlockSpec(memory_space=pltpu.HBM)
    dma = pltpu.SemaphoreType.DMA
    key_rows, value_rows, parts = pl.pallas_call(
        kernel,
        out_shape=(
            jax.ShapeDtypeStruct((1, SPAN, HD), BF16),
            jax.ShapeDtypeStruct((1, SPAN, HD), BF16),
            jax.ShapeDtypeStruct((SIDE * SIDE, 8, HD), F32),
        ),
        in_specs=[hbm] * 8,
        out_specs=(vmem, vmem, vmem),
        scratch_shapes=[
            pltpu.VMEM((1, D), F32),
            pltpu.VMEM(w_key.shape, BF16),
            pltpu.VMEM(w_value.shape, BF16),
            pltpu.VMEM((1, HD), F32),
            pltpu.VMEM(new_query.shape, BF16),
            pltpu.VMEM((1, HD), F32),
            pltpu.SMEM(stick_bias.shape, F32),
            pltpu.VMEM((SEQS, TOK, D), BF16),
            pltpu.VMEM((SEQS, 2, TOK, D), BF16),
            pltpu.VMEM((SIDE, 2 * Z, 4, 16, HD), BF16),
            pltpu.VMEM((2 * Z, PAIR, HD), BF16),
            pltpu.VMEM((CHUNKS, 8, HD), F32),
            pltpu.VMEM((16, HD), F32),
            pltpu.VMEM((8, SEQS, HD), F32),
            dma((7,)), dma((SEQS,)), dma, dma((Z,)), dma, dma, dma, dma, dma((SIDE,)), dma, dma,
            dma, dma((2, Z)), dma, dma,
        ],
        compiler_params=pltpu.CompilerParams(
            collective_id=0, has_side_effects=True, vmem_limit_bytes=40 * 2**20
        ),
    )(
        *(
            pltpu.with_memory_space_constraint(a, pltpu.HBM)
            for a in (
                tokens, in_gain.reshape(1, D), w_key, w_value, k_gain.reshape(1, HD), new_query,
                q_gain.reshape(1, HD), stick_bias,
            )
        )
    )
    return pl.pallas_call(
        write_out,
        out_shape=(
            jax.ShapeDtypeStruct((1, SPAN, HD), BF16),
            jax.ShapeDtypeStruct((1, SPAN, HD), BF16),
            jax.ShapeDtypeStruct((1, 2 * HD), F32),
        ),
        in_specs=[vmem] * 3,
        out_specs=[hbm] * 3,
        scratch_shapes=[pltpu.VMEM((1, 2 * HD), F32), dma((3, 4))],
        compiler_params=pltpu.CompilerParams(vmem_limit_bytes=40 * 2**20),
    )(key_rows, value_rows, parts)


def solution(mesh):
    return jax.shard_map(
        shards,
        mesh=mesh,
        in_specs=(
            P(None, ("sp", "tp"), None), P(), P("tp", None), P("tp", None), P(), P(), P(), P(),
        ),
        out_specs=(P("tp", "sp", None), P("tp", "sp", None), P("tp", None)),
        check_vma=False,
    )
```

```python
import functools

import jax
import jax.numpy as jnp
from jax import lax
from jax.experimental import pallas as pl
from jax.experimental.pallas import tpu as pltpu
from jax.sharding import PartitionSpec as P

MESH = pl.DeviceIdType.MESH
NORM_EPS = 1e-06
F32 = jnp.float32
BF16 = jnp.bfloat16

Z = 16
SIDE = 4
SEQS = 8
TOK = 96
PAIR = 2 * TOK
D = 2048
HD = 128
SPAN = Z * PAIR
CHUNKS = SPAN // HD


def log1p_unit(e):
    t = e / (2.0 + e)
    t2 = t * t
    acc = jnp.full_like(t, 1.0 / 15.0)
    for n in (13.0, 11.0, 9.0, 7.0, 5.0, 3.0):
        acc = acc * t2 + 1.0 / n
    return 2.0 * t * (acc * t2 + 1.0)


def first_head(second, chip_z, target_core):
    return (second + chip_z // SIDE + chip_z + target_core * 2 * (Z - chip_z)) % SIDE


def half_of(slot):
    return 0 if slot == 1 else Z


def far_first(i):
    return Z // 2 + (1 - 2 * (i % 2)) * ((i + 1) // 2)


def kernel(
    tokens_ref, in_gain_in, w_key_in, w_value_in, k_gain_in, query_in, q_gain_in, bias_in,
    key_out, value_out, parts,
    in_gain_ref, w_key_ref, w_value_ref, k_gain_ref, query_ref, q_gain_ref, bias_ref,
    raw, normed, weights, sendbuf, scores, queries, qflat,
    in_sem, tok_sem, wz_send, wz_recv, wl_sem, w1_send, w1_recv, w2_send, w2_recv, x_send, x_recv,
    kv_send, kv_recv, p_send, p_recv,
):
    sp = lax.axis_index("sp")
    tp = lax.axis_index("tp")
    z, core = tp // 2, tp % 2
    y, x = sp // SIDE, sp % SIDE
    first, second = y + core * (x - y), x + core * (y - x)
    first_step, second_step = SIDE - 3 * core, 1 + 3 * core

    barrier = pltpu.get_barrier_semaphore()

    def greet_tp(i, carry):
        pl.semaphore_signal(barrier, inc=1, device_id=(sp, (tp + i) % (2 * Z)), device_id_type=MESH)
        return carry

    def greet_sp(i, carry):
        pl.semaphore_signal(barrier, inc=1, device_id=((sp + i) % (SIDE * SIDE), tp), device_id_type=MESH)
        return carry

    lax.fori_loop(1, 2 * Z, greet_tp, 0)
    lax.fori_loop(1, SIDE * SIDE, greet_sp, 0)

    fetched = [
        pltpu.make_async_copy(source, target, in_sem.at[i])
        for i, (source, target) in enumerate((
            (w_key_in, w_key_ref), (w_value_in, w_value_ref), (query_in, query_ref), (q_gain_in, q_gain_ref),
            (in_gain_in, in_gain_ref), (k_gain_in, k_gain_ref), (bias_in, bias_ref),
        ))
    ]
    for copy in fetched:
        copy.start()

    def fetch(s, carry):
        pltpu.make_async_copy(tokens_ref.at[s], raw.at[s], tok_sem.at[s]).start()
        return carry

    lax.fori_loop(0, SEQS, fetch, 0)

    for copy in fetched:
        copy.wait()

    for i in range(8):
        qflat[i] = query_ref[:, pl.ds(i * HD, HD)].astype(F32)
    group, seq = tp // SEQS, tp % SEQS
    queries[...] = jnp.zeros_like(queries)
    for i in range(2):
        head = qflat[group * 2 + i, pl.ds(seq, 1), :]
        inverse = lax.rsqrt(jnp.mean(head * head, axis=-1, keepdims=True) + NORM_EPS)
        head = head * inverse * q_gain_ref[...]
        queries[pl.ds(i, 1), :] = head
        queries[pl.ds(i + 2, 1), :] = head

    with jax.named_scope("barrier"):
        pl.semaphore_wait(barrier, 2 * Z - 1 + SIDE * SIDE - 1)

    def tile_of(target_core, to_z):
        ref = (w_key_ref, w_value_ref)[target_core]
        rows, head = (y, x)[target_core], first_head((x, y)[target_core], to_z, target_core)
        return ref.at[pl.ds(pl.multiple_of(rows * 16, 16), 16), pl.ds(pl.multiple_of(head * HD, HD), HD)]

    def landing(target_core):
        return weights.at[0, tp, (y, x)[target_core]]

    def deal(target_core, i, carry):
        to_z = (z + far_first(i)) % Z
        pltpu.make_async_remote_copy(
            tile_of(target_core, to_z), landing(target_core), wz_send, wz_recv.at[z],
            device_id=(sp, to_z * 2 + target_core), device_id_type=MESH,
        ).start()
        return carry

    def deal_all(target_core):
        with jax.named_scope("deal"):
            lax.fori_loop(0, Z - 1, functools.partial(deal, target_core), 0)

        @pl.when(core == target_core)
        def _():
            pltpu.make_async_copy(tile_of(target_core, z), landing(target_core), wl_sem).start()

        @pl.when(core != target_core)
        def _():
            pltpu.make_async_remote_copy(
                tile_of(target_core, z), landing(target_core), wz_send, wz_recv.at[z],
                device_id=(sp, z * 2 + target_core), device_id_type=MESH,
            ).start()

    deal_all(0)

    def norm(s, carry):
        pltpu.make_async_copy(tokens_ref.at[s], raw.at[s], tok_sem.at[s]).wait()
        for part in range(TOK // 16):
            rows = raw[s, pl.ds(part * 16, 16), :].astype(F32)
            inverse = lax.rsqrt(jnp.mean(rows * rows, axis=-1, keepdims=True) + NORM_EPS)
            normed[s, core, pl.ds(part * 16, 16), :] = (rows * inverse * in_gain_ref[...]).astype(BF16)
        pltpu.make_async_remote_copy(
            normed.at[s, core], normed.at[s, core], x_send, x_recv,
            device_id=(sp, z * 2 + 1 - core), device_id_type=MESH,
        ).start()
        return carry

    with jax.named_scope("norm"):
        lax.fori_loop(0, SEQS, norm, 0)

    deal_all(1)

    def sp_of(a, b):
        return a * first_step + b * second_step

    def pass_on(from_z):
        tiles = weights.at[0, pl.ds(from_z * 2, 2), first]
        for i in (2, 1, 3):
            pltpu.make_async_remote_copy(
                tiles, tiles, w1_send, w1_recv,
                device_id=(sp_of((first + i) % SIDE, second), tp), device_id_type=MESH,
            ).start()

    one, two = weights.at[0, 0, 0], weights.at[0, pl.ds(0, 2), 0]

    def forward(i, carry):
        from_z = (z + far_first(Z - 2 - i)) % Z
        pltpu.make_async_copy(two, two, wz_recv.at[from_z]).wait()
        pass_on(from_z)
        return carry

    with jax.named_scope("z_phase"):
        pltpu.make_async_copy(one, one, wl_sem).wait()
        pltpu.make_async_copy(one, one, wz_recv.at[z]).wait()
        pass_on(z)
        lax.fori_loop(0, Z - 1, forward, 0)
    three = weights.at[0, :, pl.ds(0, 3)]
    with jax.named_scope("first_phase"):
        pltpu.make_async_copy(three, three, w1_recv).wait()

    def hand(source, slot, from_slot):
        target = weights.at[slot, pl.ds(half_of(from_slot), Z)] if slot == 2 else weights.at[slot]
        pltpu.make_async_remote_copy(
            source, target, w2_send, w2_recv.at[slot],
            device_id=(sp_of(first, (second + SIDE + from_slot - slot) % SIDE), tp), device_id_type=MESH,
        ).start()

    for slot in (1, 3):
        hand(weights.at[0], slot, 0)

    half = normed.at[:, 0]
    with jax.named_scope("partner"):
        pltpu.make_async_copy(half, half, x_recv).wait()

    def project(slot, i):
        head = (first_head(second, z, core) + slot) % SIDE
        around = (head + SIDE - z // SIDE) % SIDE
        odd, back = around % 2, around // 2
        chip = odd * ((1 - back) * (3 - i) + back * i) + (1 - odd) * (i % 2 * (3 - i // 2) + (1 - i % 2) * (i // 2))
        for half_at in range(2):
            s = chip * 2 + (core + half_at) % 2
            raw_rows = jnp.dot(
                normed[s].reshape(PAIR, D), weights[slot].reshape(D, HD), preferred_element_type=F32
            )
            inverse = lax.rsqrt(jnp.mean(raw_rows * raw_rows, axis=-1, keepdims=True) + NORM_EPS)
            out = jnp.where(core == 0, raw_rows * inverse * k_gain_ref[...], raw_rows)
            sendbuf[slot * SEQS + s] = out.astype(BF16)
            target = head * SEQS + s
            source = sendbuf.at[slot * SEQS + s]
            for which, out_ref in enumerate((key_out, value_out)):
                there = out_ref.at[0, pl.ds(pl.multiple_of(z * PAIR, PAIR), PAIR)]

                @pl.when(jnp.logical_and(core == which, target == tp))
                def _():
                    pltpu.make_async_copy(source, there, kv_recv.at[which, z]).start()

                @pl.when(jnp.logical_and(core == which, target != tp))
                def _():
                    pltpu.make_async_remote_copy(
                        source, there, kv_send, kv_recv.at[which, z],
                        device_id=(sp, target), device_id_type=MESH,
                    ).start()

    def project_slot(slot, n, carry):
        project(slot, n)
        return carry

    with jax.named_scope("project"):
        lax.fori_loop(0, SIDE, functools.partial(project_slot, 0), 0)
    for slot in (1, 3):
        with jax.named_scope("slot"):
            pltpu.make_async_copy(weights.at[slot], weights.at[slot], w2_recv.at[slot]).wait()
        hand(weights.at[slot, pl.ds(half_of(slot), Z)], 2, slot)

    off = (first_head(second, z, core) + SIDE - z // SIDE) % SIDE
    odd, upper = off % 2, off // 2

    def third(turn, n, carry):
        both_slot, both_at = 1 + 2 * (n % 2), n // 2
        if turn == 0:
            slot, at = odd * off + (1 - odd) * both_slot, odd * n + (1 - odd) * both_at
        elif turn == 1:
            both = (1 - odd) * upper
            slot, at = both * both_slot + (1 - both) * 2, both * (both_at + 2) + (1 - both) * n
        else:
            both, two = (1 - odd) * (1 - upper), (1 - odd) * upper
            slot = both * both_slot + two * 2 + odd * (SIDE - off)
            at = both * (both_at + 2) + (1 - both) * n
        project(slot, at)
        return carry

    for turn in range(3):
        if turn == 1:
            with jax.named_scope("slot"):
                pltpu.make_async_copy(weights.at[2], weights.at[2], w2_recv.at[2]).wait()
        with jax.named_scope("project"):
            lax.fori_loop(0, SIDE, functools.partial(third, turn), 0)

    query = queries[...].astype(BF16)

    def score(pair, carry):
        for i in range(2):
            at = pair * 2 + i
            block = key_out.at[0, pl.ds(pl.multiple_of(at * PAIR, PAIR), PAIR)]
            pltpu.make_async_copy(block, block, kv_recv.at[0, at]).wait()
        for i in range(3):
            chunk = pair * 3 + i
            keys = key_out[0, pl.ds(pl.multiple_of(chunk * HD, HD), HD), :]
            scores[chunk] = lax.dot_general(query, keys, (((1,), (1,)), ((), ())), preferred_element_type=F32)[:8]
        return carry

    with jax.named_scope("score"):
        lax.fori_loop(0, Z // 2, score, 0)

    row = lax.broadcasted_iota(jnp.int32, (1, 8, HD), 1)
    bias = jnp.where(row % 2 == 0, bias_ref[group * 2], bias_ref[group * 2 + 1])
    score_all = scores[...] * (HD ** -0.5) + bias
    soft = log1p_unit(jnp.exp(-jnp.abs(score_all)))
    log_keep = -(jnp.maximum(score_all, 0.0) + soft)
    log_take = -(jnp.maximum(-score_all, 0.0) + soft)
    later = (
        lax.broadcasted_iota(jnp.int32, (HD, HD), 0) > lax.broadcasted_iota(jnp.int32, (HD, HD), 1)
    ).astype(F32)
    after = jnp.dot(
        log_keep.reshape(CHUNKS * 8, HD), later, preferred_element_type=F32, precision=lax.Precision.HIGHEST
    ).reshape(CHUNKS, 8, HD)
    totals = jnp.sum(log_keep, axis=2, keepdims=True)
    carried = jnp.zeros((8, 1), F32)
    chunk_weights = [None] * CHUNKS
    for chunk in reversed(range(CHUNKS)):
        chunk_weights[chunk] = jnp.exp(log_take[chunk] + after[chunk] + carried).astype(BF16)
        carried = carried + totals[chunk]

    def arrive(at, carry):
        block = value_out.at[0, pl.ds(pl.multiple_of(at * PAIR, PAIR), PAIR)]
        pltpu.make_async_copy(block, block, kv_recv.at[1, at]).wait()
        return carry

    with jax.named_scope("arrive"):
        lax.fori_loop(0, Z, arrive, 0)
    partial = jnp.zeros((8, HD), F32)
    for chunk in range(CHUNKS):
        partial = partial + jnp.dot(
            chunk_weights[chunk], value_out[0, pl.ds(chunk * HD, HD), :], preferred_element_type=F32
        )

    parts[sp] = jnp.where(row[0] < 2, partial, carried)

    def share(i, carry):
        pltpu.make_async_remote_copy(
            parts.at[sp], parts.at[sp], p_send, p_recv,
            device_id=((sp + i) % (SIDE * SIDE), tp), device_id_type=MESH,
        ).start()
        return carry

    lax.fori_loop(1, SIDE * SIDE, share, 0)
    others = parts.at[pl.ds(0, SIDE * SIDE - 1)]
    with jax.named_scope("others"):
        pltpu.make_async_copy(others, others, p_recv).wait()
    column = weights.at[0, pl.ds(0, 2 * Z - 1), 0]
    pltpu.make_async_copy(column, column, wz_send).wait()
    pltpu.make_async_copy(three, three, w1_send).wait()
    pltpu.make_async_copy(weights.at[pl.ds(0, 3)], weights.at[pl.ds(0, 3)], w2_send).wait()
    pltpu.make_async_copy(half, half, x_send).wait()

    sent = sendbuf.at[pl.ds(0, 2 * Z - 1)]
    with jax.named_scope("drain"):
        pltpu.make_async_copy(sent, sent, kv_send).wait()
    pltpu.make_async_copy(others, others, p_send).wait()


def write_out(key_ref, value_ref, parts_ref, key_out, value_out, read_out, read, sems):
    copies = [
        pltpu.make_async_copy(ref.at[0, pl.ds(i * (SPAN // 4), SPAN // 4)], out.at[0, pl.ds(i * (SPAN // 4), SPAN // 4)], sems.at[n, i])
        for n, (ref, out) in enumerate(((key_ref, key_out), (value_ref, value_out)))
        for i in range(4)
    ]
    for copy in copies:
        copy.start()
    total = jnp.zeros((2, HD), F32)
    log_later = jnp.zeros((2, HD), F32)
    for span in reversed(range(SIDE * SIDE)):
        total = total + jnp.exp(log_later) * parts_ref[span, pl.ds(0, 2), :]
        log_later = log_later + parts_ref[span, pl.ds(2, 2), :]
    read[:, pl.ds(0, HD)] = total[0:1]
    read[:, pl.ds(HD, HD)] = total[1:2]
    last = pltpu.make_async_copy(read, read_out, sems.at[2, 0])
    last.start()
    for copy in copies:
        copy.wait()
    last.wait()


def shards(tokens, in_gain, w_key, w_value, k_gain, new_query, q_gain, stick_bias):
    vmem = pl.BlockSpec(memory_space=pltpu.VMEM)
    hbm = pl.BlockSpec(memory_space=pltpu.HBM)
    dma = pltpu.SemaphoreType.DMA
    key_rows, value_rows, parts = pl.pallas_call(
        kernel,
        out_shape=(
            jax.ShapeDtypeStruct((1, SPAN, HD), BF16),
            jax.ShapeDtypeStruct((1, SPAN, HD), BF16),
            jax.ShapeDtypeStruct((SIDE * SIDE, 8, HD), F32),
        ),
        in_specs=[hbm] * 8,
        out_specs=(vmem, vmem, vmem),
        scratch_shapes=[
            pltpu.VMEM((1, D), F32),
            pltpu.VMEM(w_key.shape, BF16),
            pltpu.VMEM(w_value.shape, BF16),
            pltpu.VMEM((1, HD), F32),
            pltpu.VMEM(new_query.shape, BF16),
            pltpu.VMEM((1, HD), F32),
            pltpu.SMEM(stick_bias.shape, F32),
            pltpu.VMEM((SEQS, TOK, D), BF16),
            pltpu.VMEM((SEQS, 2, TOK, D), BF16),
            pltpu.VMEM((SIDE, 2 * Z, 4, 16, HD), BF16),
            pltpu.VMEM((2 * Z, PAIR, HD), BF16),
            pltpu.VMEM((CHUNKS, 8, HD), F32),
            pltpu.VMEM((16, HD), F32),
            pltpu.VMEM((8, SEQS, HD), F32),
            dma((7,)), dma((SEQS,)), dma, dma((Z,)), dma, dma, dma, dma, dma((SIDE,)), dma, dma,
            dma, dma((2, Z)), dma, dma,
        ],
        compiler_params=pltpu.CompilerParams(
            collective_id=0, has_side_effects=True, vmem_limit_bytes=40 * 2**20
        ),
    )(
        *(
            pltpu.with_memory_space_constraint(a, pltpu.HBM)
            for a in (
                tokens, in_gain.reshape(1, D), w_key, w_value, k_gain.reshape(1, HD), new_query,
                q_gain.reshape(1, HD), stick_bias,
            )
        )
    )
    return pl.pallas_call(
        write_out,
        out_shape=(
            jax.ShapeDtypeStruct((1, SPAN, HD), BF16),
            jax.ShapeDtypeStruct((1, SPAN, HD), BF16),
            jax.ShapeDtypeStruct((1, 2 * HD), F32),
        ),
        in_specs=[vmem] * 3,
        out_specs=[hbm] * 3,
        scratch_shapes=[pltpu.VMEM((1, 2 * HD), F32), dma((3, 4))],
        compiler_params=pltpu.CompilerParams(vmem_limit_bytes=40 * 2**20),
    )(key_rows, value_rows, parts)


def solution(mesh):
    return jax.shard_map(
        shards,
        mesh=mesh,
        in_specs=(
            P(None, ("sp", "tp"), None), P(), P("tp", None), P("tp", None), P(), P(), P(), P(),
        ),
        out_specs=(P("tp", "sp", None), P("tp", "sp", None), P("tp", None)),
        check_vma=False,
    )
```

```python
import functools

import jax
import jax.numpy as jnp
from jax import lax
from jax.experimental import pallas as pl
from jax.experimental.pallas import tpu as pltpu
from jax.sharding import PartitionSpec as P

MESH = pl.DeviceIdType.MESH
NORM_EPS = 1e-06
F32 = jnp.float32
BF16 = jnp.bfloat16

Z = 16
SIDE = 4
SEQS = 8
TOK = 96
PAIR = 2 * TOK
D = 2048
HD = 128
SPAN = Z * PAIR
CHUNKS = SPAN // HD


def log1p_unit(e):
    t = e / (2.0 + e)
    t2 = t * t
    acc = jnp.full_like(t, 1.0 / 15.0)
    for n in (13.0, 11.0, 9.0, 7.0, 5.0, 3.0):
        acc = acc * t2 + 1.0 / n
    return 2.0 * t * (acc * t2 + 1.0)


def first_head(second, chip_z, target_core):
    return (second + chip_z // SIDE + chip_z + target_core * 2 * (Z - chip_z)) % SIDE


def half_of(slot):
    return 0 if slot == 1 else Z


def far_first(i):
    return Z // 2 + (1 - 2 * (i % 2)) * ((i + 1) // 2)


def kernel(
    tokens_ref, in_gain_in, w_key_in, w_value_in, k_gain_in, query_in, q_gain_in, bias_in,
    key_out, value_out, parts,
    in_gain_ref, w_key_ref, w_value_ref, k_gain_ref, query_ref, q_gain_ref, bias_ref,
    raw, normed, weights, sendbuf, scores, queries, qflat,
    in_sem, tok_sem, wz_send, wz_recv, wl_sem, w1_send, w1_recv, w2_send, w2_recv, x_send, x_recv,
    kv_send, kv_recv, p_send, p_recv,
):
    sp = lax.axis_index("sp")
    tp = lax.axis_index("tp")
    z, core = tp // 2, tp % 2
    y, x = sp // SIDE, sp % SIDE
    first, second = y + core * (x - y), x + core * (y - x)
    first_step, second_step = SIDE - 3 * core, 1 + 3 * core

    barrier = pltpu.get_barrier_semaphore()

    def greet_tp(i, carry):
        pl.semaphore_signal(barrier, inc=1, device_id=(sp, (tp + i) % (2 * Z)), device_id_type=MESH)
        return carry

    def greet_sp(i, carry):
        pl.semaphore_signal(barrier, inc=1, device_id=((sp + i) % (SIDE * SIDE), tp), device_id_type=MESH)
        return carry

    lax.fori_loop(1, 2 * Z, greet_tp, 0)
    lax.fori_loop(1, SIDE * SIDE, greet_sp, 0)

    fetched = [
        pltpu.make_async_copy(source, target, in_sem.at[i])
        for i, (source, target) in enumerate((
            (w_key_in, w_key_ref), (w_value_in, w_value_ref), (query_in, query_ref), (q_gain_in, q_gain_ref),
            (in_gain_in, in_gain_ref), (k_gain_in, k_gain_ref), (bias_in, bias_ref),
        ))
    ]
    for copy in fetched:
        copy.start()

    def fetch(s, carry):
        pltpu.make_async_copy(tokens_ref.at[s], raw.at[s], tok_sem.at[s]).start()
        return carry

    lax.fori_loop(0, SEQS, fetch, 0)

    for copy in fetched:
        copy.wait()

    for i in range(8):
        qflat[i] = query_ref[:, pl.ds(i * HD, HD)].astype(F32)
    group, seq = tp // SEQS, tp % SEQS
    queries[...] = jnp.zeros_like(queries)
    for i in range(2):
        head = qflat[group * 2 + i, pl.ds(seq, 1), :]
        inverse = lax.rsqrt(jnp.mean(head * head, axis=-1, keepdims=True) + NORM_EPS)
        head = head * inverse * q_gain_ref[...]
        queries[pl.ds(i, 1), :] = head
        queries[pl.ds(i + 2, 1), :] = head

    with jax.named_scope("barrier"):
        pl.semaphore_wait(barrier, 2 * Z - 1 + SIDE * SIDE - 1)

    def tile_of(target_core, to_z):
        ref = (w_key_ref, w_value_ref)[target_core]
        rows, head = (y, x)[target_core], first_head((x, y)[target_core], to_z, target_core)
        return ref.at[pl.ds(pl.multiple_of(rows * 16, 16), 16), pl.ds(pl.multiple_of(head * HD, HD), HD)]

    def landing(target_core):
        return weights.at[0, tp, (y, x)[target_core]]

    def deal(target_core, i, carry):
        to_z = (z + far_first(i)) % Z
        pltpu.make_async_remote_copy(
            tile_of(target_core, to_z), landing(target_core), wz_send, wz_recv.at[z],
            device_id=(sp, to_z * 2 + target_core), device_id_type=MESH,
        ).start()
        return carry

    def deal_all(target_core):
        with jax.named_scope("deal"):
            lax.fori_loop(0, Z - 1, functools.partial(deal, target_core), 0)

        @pl.when(core == target_core)
        def _():
            pltpu.make_async_copy(tile_of(target_core, z), landing(target_core), wl_sem).start()

        @pl.when(core != target_core)
        def _():
            pltpu.make_async_remote_copy(
                tile_of(target_core, z), landing(target_core), wz_send, wz_recv.at[z],
                device_id=(sp, z * 2 + target_core), device_id_type=MESH,
            ).start()

    deal_all(0)

    def norm(s, carry):
        pltpu.make_async_copy(tokens_ref.at[s], raw.at[s], tok_sem.at[s]).wait()
        for part in range(TOK // 16):
            rows = raw[s, pl.ds(part * 16, 16), :].astype(F32)
            inverse = lax.rsqrt(jnp.mean(rows * rows, axis=-1, keepdims=True) + NORM_EPS)
            normed[s, core, pl.ds(part * 16, 16), :] = (rows * inverse * in_gain_ref[...]).astype(BF16)
        pltpu.make_async_remote_copy(
            normed.at[s, core], normed.at[s, core], x_send, x_recv,
            device_id=(sp, z * 2 + 1 - core), device_id_type=MESH,
        ).start()
        return carry

    with jax.named_scope("norm"):
        lax.fori_loop(0, SEQS, norm, 0)

    deal_all(1)

    def sp_of(a, b):
        return a * first_step + b * second_step

    def pass_on(from_z):
        tiles = weights.at[0, pl.ds(from_z * 2, 2), first]
        for i in (2, 1, 3):
            pltpu.make_async_remote_copy(
                tiles, tiles, w1_send, w1_recv,
                device_id=(sp_of((first + i) % SIDE, second), tp), device_id_type=MESH,
            ).start()

    one, two = weights.at[0, 0, 0], weights.at[0, pl.ds(0, 2), 0]

    def forward(i, carry):
        from_z = (z + far_first(Z - 2 - i)) % Z
        pltpu.make_async_copy(two, two, wz_recv.at[from_z]).wait()
        pass_on(from_z)
        return carry

    with jax.named_scope("z_phase"):
        pltpu.make_async_copy(one, one, wl_sem).wait()
        pltpu.make_async_copy(one, one, wz_recv.at[z]).wait()
        pass_on(z)
        lax.fori_loop(0, Z - 1, forward, 0)

    def hand(source, target, slot, from_slot):
        pltpu.make_async_remote_copy(
            source, target, w2_send, w2_recv.at[slot],
            device_id=(sp_of(first, (second + SIDE + from_slot - slot) % SIDE), tp), device_id_type=MESH,
        ).start()

    for slot in (1, 3):
        hand(weights.at[0, :, first], weights.at[slot, :, first], slot, 0)
    three = weights.at[0, :, pl.ds(0, 3)]
    with jax.named_scope("first_phase"):
        pltpu.make_async_copy(three, three, w1_recv).wait()
    for i in range(1, SIDE):
        rows = (first + i) % SIDE
        for slot in (1, 3):
            hand(weights.at[0, :, rows], weights.at[slot, :, rows], slot, 0)

    half = normed.at[:, 0]
    with jax.named_scope("partner"):
        pltpu.make_async_copy(half, half, x_recv).wait()

    def project(slot, i):
        head = (first_head(second, z, core) + slot) % SIDE
        around = (head + SIDE - z // SIDE) % SIDE
        odd, back = around % 2, around // 2
        chip = odd * ((1 - back) * (3 - i) + back * i) + (1 - odd) * (i % 2 * (3 - i // 2) + (1 - i % 2) * (i // 2))
        both = pl.ds(chip * 2, 2)
        raw_rows = jnp.dot(
            normed[both].reshape(2 * PAIR, D), weights[slot].reshape(D, HD), preferred_element_type=F32
        )
        inverse = lax.rsqrt(jnp.mean(raw_rows * raw_rows, axis=-1, keepdims=True) + NORM_EPS)
        out = jnp.where(core == 0, raw_rows * inverse * k_gain_ref[...], raw_rows)
        sendbuf[pl.ds(slot * SEQS + chip * 2, 2)] = out.astype(BF16).reshape(2, PAIR, HD)
        for half_at in range(2):
            s = chip * 2 + (core + half_at) % 2
            target = head * SEQS + s
            source = sendbuf.at[slot * SEQS + s]
            for which, out_ref in enumerate((key_out, value_out)):
                there = out_ref.at[0, pl.ds(pl.multiple_of(z * PAIR, PAIR), PAIR)]

                @pl.when(jnp.logical_and(core == which, target == tp))
                def _():
                    pltpu.make_async_copy(source, there, kv_recv.at[which, z]).start()

                @pl.when(jnp.logical_and(core == which, target != tp))
                def _():
                    pltpu.make_async_remote_copy(
                        source, there, kv_send, kv_recv.at[which, z],
                        device_id=(sp, target), device_id_type=MESH,
                    ).start()

    def project_slot(slot, n, carry):
        project(slot, n)
        return carry

    with jax.named_scope("project"):
        lax.fori_loop(0, SIDE, functools.partial(project_slot, 0), 0)
    for slot in (1, 3):
        with jax.named_scope("slot"):
            pltpu.make_async_copy(weights.at[slot], weights.at[slot], w2_recv.at[slot]).wait()
        half_rows = pl.ds(half_of(slot), Z)
        hand(weights.at[slot, half_rows], weights.at[2, half_rows], 2, slot)

    off = (first_head(second, z, core) + SIDE - z // SIDE) % SIDE
    odd, upper = off % 2, off // 2

    def third(turn, n, carry):
        both_slot, both_at = 1 + 2 * (n % 2), n // 2
        if turn == 0:
            slot, at = odd * off + (1 - odd) * both_slot, odd * n + (1 - odd) * both_at
        elif turn == 1:
            both = (1 - odd) * upper
            slot, at = both * both_slot + (1 - both) * 2, both * (both_at + 2) + (1 - both) * n
        else:
            both, two = (1 - odd) * (1 - upper), (1 - odd) * upper
            slot = both * both_slot + two * 2 + odd * (SIDE - off)
            at = both * (both_at + 2) + (1 - both) * n
        project(slot, at)
        return carry

    for turn in range(3):
        if turn == 1:
            with jax.named_scope("slot"):
                pltpu.make_async_copy(weights.at[2], weights.at[2], w2_recv.at[2]).wait()
        with jax.named_scope("project"):
            lax.fori_loop(0, SIDE, functools.partial(third, turn), 0)

    query = queries[...].astype(BF16)

    def score(pair, carry):
        for i in range(2):
            at = pair * 2 + i
            block = key_out.at[0, pl.ds(pl.multiple_of(at * PAIR, PAIR), PAIR)]
            pltpu.make_async_copy(block, block, kv_recv.at[0, at]).wait()
        for i in range(3):
            chunk = pair * 3 + i
            keys = key_out[0, pl.ds(pl.multiple_of(chunk * HD, HD), HD), :]
            scores[chunk] = lax.dot_general(query, keys, (((1,), (1,)), ((), ())), preferred_element_type=F32)[:8]
        return carry

    with jax.named_scope("score"):
        lax.fori_loop(0, Z // 2, score, 0)

    row = lax.broadcasted_iota(jnp.int32, (1, 8, HD), 1)
    bias = jnp.where(row % 2 == 0, bias_ref[group * 2], bias_ref[group * 2 + 1])
    score_all = scores[...] * (HD ** -0.5) + bias
    soft = log1p_unit(jnp.exp(-jnp.abs(score_all)))
    log_keep = -(jnp.maximum(score_all, 0.0) + soft)
    log_take = -(jnp.maximum(-score_all, 0.0) + soft)
    later = (
        lax.broadcasted_iota(jnp.int32, (HD, HD), 0) > lax.broadcasted_iota(jnp.int32, (HD, HD), 1)
    ).astype(F32)
    after = jnp.dot(
        log_keep.reshape(CHUNKS * 8, HD), later, preferred_element_type=F32, precision=lax.Precision.HIGHEST
    ).reshape(CHUNKS, 8, HD)
    totals = jnp.sum(log_keep, axis=2, keepdims=True)
    carried = jnp.zeros((8, 1), F32)
    chunk_weights = [None] * CHUNKS
    for chunk in reversed(range(CHUNKS)):
        chunk_weights[chunk] = jnp.exp(log_take[chunk] + after[chunk] + carried).astype(BF16)
        carried = carried + totals[chunk]

    def arrive(at, carry):
        block = value_out.at[0, pl.ds(pl.multiple_of(at * PAIR, PAIR), PAIR)]
        pltpu.make_async_copy(block, block, kv_recv.at[1, at]).wait()
        return carry

    with jax.named_scope("arrive"):
        lax.fori_loop(0, Z, arrive, 0)
    partial = jnp.zeros((8, HD), F32)
    for chunk in range(CHUNKS):
        partial = partial + jnp.dot(
            chunk_weights[chunk], value_out[0, pl.ds(chunk * HD, HD), :], preferred_element_type=F32
        )

    parts[sp] = jnp.where(row[0] < 2, partial, carried)

    def share(i, carry):
        pltpu.make_async_remote_copy(
            parts.at[sp], parts.at[sp], p_send, p_recv,
            device_id=((sp + i) % (SIDE * SIDE), tp), device_id_type=MESH,
        ).start()
        return carry

    lax.fori_loop(1, SIDE * SIDE, share, 0)
    others = parts.at[pl.ds(0, SIDE * SIDE - 1)]
    with jax.named_scope("others"):
        pltpu.make_async_copy(others, others, p_recv).wait()
    column = weights.at[0, pl.ds(0, 2 * Z - 1), 0]
    pltpu.make_async_copy(column, column, wz_send).wait()
    pltpu.make_async_copy(three, three, w1_send).wait()
    pltpu.make_async_copy(weights.at[pl.ds(0, 3)], weights.at[pl.ds(0, 3)], w2_send).wait()
    pltpu.make_async_copy(half, half, x_send).wait()

    sent = sendbuf.at[pl.ds(0, 2 * Z - 1)]
    with jax.named_scope("drain"):
        pltpu.make_async_copy(sent, sent, kv_send).wait()
    pltpu.make_async_copy(others, others, p_send).wait()


def write_out(key_ref, value_ref, parts_ref, key_out, value_out, read_out, read, sems):
    copies = [
        pltpu.make_async_copy(ref.at[0, pl.ds(i * (SPAN // 4), SPAN // 4)], out.at[0, pl.ds(i * (SPAN // 4), SPAN // 4)], sems.at[n, i])
        for n, (ref, out) in enumerate(((key_ref, key_out), (value_ref, value_out)))
        for i in range(4)
    ]
    for copy in copies:
        copy.start()
    total = jnp.zeros((2, HD), F32)
    log_later = jnp.zeros((2, HD), F32)
    for span in reversed(range(SIDE * SIDE)):
        total = total + jnp.exp(log_later) * parts_ref[span, pl.ds(0, 2), :]
        log_later = log_later + parts_ref[span, pl.ds(2, 2), :]
    read[:, pl.ds(0, HD)] = total[0:1]
    read[:, pl.ds(HD, HD)] = total[1:2]
    last = pltpu.make_async_copy(read, read_out, sems.at[2, 0])
    last.start()
    for copy in copies:
        copy.wait()
    last.wait()


def shards(tokens, in_gain, w_key, w_value, k_gain, new_query, q_gain, stick_bias):
    vmem = pl.BlockSpec(memory_space=pltpu.VMEM)
    hbm = pl.BlockSpec(memory_space=pltpu.HBM)
    dma = pltpu.SemaphoreType.DMA
    key_rows, value_rows, parts = pl.pallas_call(
        kernel,
        out_shape=(
            jax.ShapeDtypeStruct((1, SPAN, HD), BF16),
            jax.ShapeDtypeStruct((1, SPAN, HD), BF16),
            jax.ShapeDtypeStruct((SIDE * SIDE, 8, HD), F32),
        ),
        in_specs=[hbm] * 8,
        out_specs=(vmem, vmem, vmem),
        scratch_shapes=[
            pltpu.VMEM((1, D), F32),
            pltpu.VMEM(w_key.shape, BF16),
            pltpu.VMEM(w_value.shape, BF16),
            pltpu.VMEM((1, HD), F32),
            pltpu.VMEM(new_query.shape, BF16),
            pltpu.VMEM((1, HD), F32),
            pltpu.SMEM(stick_bias.shape, F32),
            pltpu.VMEM((SEQS, TOK, D), BF16),
            pltpu.VMEM((SEQS, 2, TOK, D), BF16),
            pltpu.VMEM((SIDE, 2 * Z, 4, 16, HD), BF16),
            pltpu.VMEM((2 * Z, PAIR, HD), BF16),
            pltpu.VMEM((CHUNKS, 8, HD), F32),
            pltpu.VMEM((16, HD), F32),
            pltpu.VMEM((8, SEQS, HD), F32),
            dma((7,)), dma((SEQS,)), dma, dma((Z,)), dma, dma, dma, dma, dma((SIDE,)), dma, dma,
            dma, dma((2, Z)), dma, dma,
        ],
        compiler_params=pltpu.CompilerParams(
            collective_id=0, has_side_effects=True, vmem_limit_bytes=40 * 2**20
        ),
    )(
        *(
            pltpu.with_memory_space_constraint(a, pltpu.HBM)
            for a in (
                tokens, in_gain.reshape(1, D), w_key, w_value, k_gain.reshape(1, HD), new_query,
                q_gain.reshape(1, HD), stick_bias,
            )
        )
    )
    return pl.pallas_call(
        write_out,
        out_shape=(
            jax.ShapeDtypeStruct((1, SPAN, HD), BF16),
            jax.ShapeDtypeStruct((1, SPAN, HD), BF16),
            jax.ShapeDtypeStruct((1, 2 * HD), F32),
        ),
        in_specs=[vmem] * 3,
        out_specs=[hbm] * 3,
        scratch_shapes=[pltpu.VMEM((1, 2 * HD), F32), dma((3, 4))],
        compiler_params=pltpu.CompilerParams(vmem_limit_bytes=40 * 2**20),
    )(key_rows, value_rows, parts)


def solution(mesh):
    return jax.shard_map(
        shards,
        mesh=mesh,
        in_specs=(
            P(None, ("sp", "tp"), None), P(), P("tp", None), P("tp", None), P(), P(), P(), P(),
        ),
        out_specs=(P("tp", "sp", None), P("tp", "sp", None), P("tp", None)),
        check_vma=False,
    )
```

```python
import functools

import jax
import jax.numpy as jnp
from jax import lax
from jax.experimental import pallas as pl
from jax.experimental.pallas import tpu as pltpu
from jax.sharding import PartitionSpec as P

MESH = pl.DeviceIdType.MESH
NORM_EPS = 1e-06
F32 = jnp.float32
BF16 = jnp.bfloat16

Z = 16
SIDE = 4
SEQS = 8
TOK = 96
PAIR = 2 * TOK
D = 2048
HD = 128
SPAN = Z * PAIR
CHUNKS = SPAN // HD


def log1p_unit(e):
    t = e / (2.0 + e)
    t2 = t * t
    acc = jnp.full_like(t, 1.0 / 15.0)
    for n in (13.0, 11.0, 9.0, 7.0, 5.0, 3.0):
        acc = acc * t2 + 1.0 / n
    return 2.0 * t * (acc * t2 + 1.0)


def first_head(second, chip_z, target_core):
    return (second + chip_z // SIDE + chip_z + target_core * 2 * (Z - chip_z)) % SIDE


def half_of(slot):
    return 0 if slot == 1 else Z


def far_first(i):
    return Z // 2 + (1 - 2 * (i % 2)) * ((i + 1) // 2)


def kernel(
    tokens_ref, in_gain_in, w_key_in, w_value_in, k_gain_in, query_in, q_gain_in, bias_in,
    key_out, value_out, parts,
    in_gain_ref, w_key_ref, w_value_ref, k_gain_ref, query_ref, q_gain_ref, bias_ref,
    raw, normed, weights, sendbuf, scores, queries, qflat,
    in_sem, tok_sem, wz_send, wz_recv, wl_sem, w1_send, w1_recv, w2_send, w2_recv, x_send, x_recv,
    kv_send, kv_recv, p_send, p_recv,
):
    sp = lax.axis_index("sp")
    tp = lax.axis_index("tp")
    z, core = tp // 2, tp % 2
    y, x = sp // SIDE, sp % SIDE
    first, second = y + core * (x - y), x + core * (y - x)
    first_step, second_step = SIDE - 3 * core, 1 + 3 * core

    barrier = pltpu.get_barrier_semaphore()

    def greet_tp(i, carry):
        pl.semaphore_signal(barrier, inc=1, device_id=(sp, (tp + i) % (2 * Z)), device_id_type=MESH)
        return carry

    def greet_sp(i, carry):
        pl.semaphore_signal(barrier, inc=1, device_id=((sp + i) % (SIDE * SIDE), tp), device_id_type=MESH)
        return carry

    lax.fori_loop(1, 2 * Z, greet_tp, 0)
    lax.fori_loop(1, SIDE * SIDE, greet_sp, 0)

    fetched = [
        pltpu.make_async_copy(source, target, in_sem.at[i])
        for i, (source, target) in enumerate((
            (w_key_in, w_key_ref), (w_value_in, w_value_ref), (query_in, query_ref), (q_gain_in, q_gain_ref),
            (in_gain_in, in_gain_ref), (k_gain_in, k_gain_ref), (bias_in, bias_ref),
        ))
    ]
    for copy in fetched:
        copy.start()

    def fetch(s, carry):
        pltpu.make_async_copy(tokens_ref.at[s], raw.at[s], tok_sem.at[s]).start()
        return carry

    lax.fori_loop(0, SEQS, fetch, 0)

    for copy in fetched:
        copy.wait()

    for i in range(8):
        qflat[i] = query_ref[:, pl.ds(i * HD, HD)].astype(F32)
    group, seq = tp // SEQS, tp % SEQS
    queries[...] = jnp.zeros_like(queries)
    for i in range(2):
        head = qflat[group * 2 + i, pl.ds(seq, 1), :]
        inverse = lax.rsqrt(jnp.mean(head * head, axis=-1, keepdims=True) + NORM_EPS)
        head = head * inverse * q_gain_ref[...]
        queries[pl.ds(i, 1), :] = head
        queries[pl.ds(i + 2, 1), :] = head

    with jax.named_scope("barrier"):
        pl.semaphore_wait(barrier, 2 * Z - 1 + SIDE * SIDE - 1)

    def tile_of(target_core, to_z):
        ref = (w_key_ref, w_value_ref)[target_core]
        rows, head = (y, x)[target_core], first_head((x, y)[target_core], to_z, target_core)
        return ref.at[pl.ds(pl.multiple_of(rows * 16, 16), 16), pl.ds(pl.multiple_of(head * HD, HD), HD)]

    def landing(target_core):
        return weights.at[0, tp, (y, x)[target_core]]

    def deal(target_core, i, carry):
        to_z = (z + far_first(i)) % Z
        pltpu.make_async_remote_copy(
            tile_of(target_core, to_z), landing(target_core), wz_send, wz_recv.at[z],
            device_id=(sp, to_z * 2 + target_core), device_id_type=MESH,
        ).start()
        return carry

    def deal_all(target_core):
        with jax.named_scope("deal"):
            lax.fori_loop(0, Z - 1, functools.partial(deal, target_core), 0)

        @pl.when(core == target_core)
        def _():
            pltpu.make_async_copy(tile_of(target_core, z), landing(target_core), wl_sem).start()

        @pl.when(core != target_core)
        def _():
            pltpu.make_async_remote_copy(
                tile_of(target_core, z), landing(target_core), wz_send, wz_recv.at[z],
                device_id=(sp, z * 2 + target_core), device_id_type=MESH,
            ).start()

    deal_all(0)

    def norm(s, carry):
        pltpu.make_async_copy(tokens_ref.at[s], raw.at[s], tok_sem.at[s]).wait()
        for part in range(TOK // 16):
            rows = raw[s, pl.ds(part * 16, 16), :].astype(F32)
            inverse = lax.rsqrt(jnp.mean(rows * rows, axis=-1, keepdims=True) + NORM_EPS)
            normed[s, core, pl.ds(part * 16, 16), :] = (rows * inverse * in_gain_ref[...]).astype(BF16)
        pltpu.make_async_remote_copy(
            normed.at[s, core], normed.at[s, core], x_send, x_recv,
            device_id=(sp, z * 2 + 1 - core), device_id_type=MESH,
        ).start()
        return carry

    with jax.named_scope("norm"):
        lax.fori_loop(0, SEQS, norm, 0)

    deal_all(1)

    def sp_of(a, b):
        return a * first_step + b * second_step

    def pass_on(from_z):
        tiles = weights.at[0, pl.ds(from_z * 2, 2), first]
        for i in (2, 1, 3):
            pltpu.make_async_remote_copy(
                tiles, tiles, w1_send, w1_recv,
                device_id=(sp_of((first + i) % SIDE, second), tp), device_id_type=MESH,
            ).start()

    one, two = weights.at[0, 0, 0], weights.at[0, pl.ds(0, 2), 0]

    def forward(i, carry):
        from_z = (z + far_first(Z - 2 - i)) % Z
        pltpu.make_async_copy(two, two, wz_recv.at[from_z]).wait()
        pass_on(from_z)
        return carry

    with jax.named_scope("z_phase"):
        pltpu.make_async_copy(one, one, wl_sem).wait()
        pltpu.make_async_copy(one, one, wz_recv.at[z]).wait()
        pass_on(z)
        lax.fori_loop(0, Z - 1, forward, 0)

    def hand(source, target, slot, from_slot):
        pltpu.make_async_remote_copy(
            source, target, w2_send, w2_recv.at[slot],
            device_id=(sp_of(first, (second + SIDE + from_slot - slot) % SIDE), tp), device_id_type=MESH,
        ).start()

    for slot in (1, 3):
        hand(weights.at[0, :, first], weights.at[slot, :, first], slot, 0)
    three = weights.at[0, :, pl.ds(0, 3)]
    with jax.named_scope("first_phase"):
        pltpu.make_async_copy(three, three, w1_recv).wait()
    for i in range(1, SIDE):
        rows = (first + i) % SIDE
        for slot in (1, 3):
            hand(weights.at[0, :, rows], weights.at[slot, :, rows], slot, 0)

    half = normed.at[:, 0]
    with jax.named_scope("partner"):
        pltpu.make_async_copy(half, half, x_recv).wait()

    def project(slot, i):
        head = (first_head(second, z, core) + slot) % SIDE
        around = (head + SIDE - z // SIDE) % SIDE
        odd, back = around % 2, around // 2
        chip = odd * ((1 - back) * (3 - i) + back * i) + (1 - odd) * (i % 2 * (3 - i // 2) + (1 - i % 2) * (i // 2))
        both = pl.ds(chip * 2, 2)
        raw_rows = jnp.dot(
            normed[both].reshape(2 * PAIR, D), weights[slot].reshape(D, HD), preferred_element_type=F32
        )
        inverse = lax.rsqrt(jnp.mean(raw_rows * raw_rows, axis=-1, keepdims=True) + NORM_EPS)
        out = jnp.where(core == 0, raw_rows * inverse * k_gain_ref[...], raw_rows)
        sendbuf[pl.ds(slot * SEQS + chip * 2, 2)] = out.astype(BF16).reshape(2, PAIR, HD)
        for half_at in range(2):
            s = chip * 2 + (core + half_at) % 2
            target = head * SEQS + s
            source = sendbuf.at[slot * SEQS + s]
            for which, out_ref in enumerate((key_out, value_out)):
                there = out_ref.at[0, pl.ds(pl.multiple_of(z * PAIR, PAIR), PAIR)]

                @pl.when(jnp.logical_and(core == which, target == tp))
                def _():
                    pltpu.make_async_copy(source, there, kv_recv.at[which, z]).start()

                @pl.when(jnp.logical_and(core == which, target != tp))
                def _():
                    pltpu.make_async_remote_copy(
                        source, there, kv_send, kv_recv.at[which, z],
                        device_id=(sp, target), device_id_type=MESH,
                    ).start()

    def project_slot(slot, n, carry):
        project(slot, n)
        return carry

    with jax.named_scope("project"):
        lax.fori_loop(0, SIDE, functools.partial(project_slot, 0), 0)
    for slot in (1, 3):
        with jax.named_scope("slot"):
            pltpu.make_async_copy(weights.at[slot], weights.at[slot], w2_recv.at[slot]).wait()
        half_rows = pl.ds(half_of(slot), Z)
        hand(weights.at[slot, half_rows], weights.at[2, half_rows], 2, slot)

    off = (first_head(second, z, core) + SIDE - z // SIDE) % SIDE
    odd, upper = off % 2, off // 2

    def third(turn, n, carry):
        both_slot, both_at = 1 + 2 * (n % 2), n // 2
        if turn == 0:
            slot, at = odd * off + (1 - odd) * both_slot, odd * n + (1 - odd) * both_at
        elif turn == 1:
            both = (1 - odd) * upper
            slot, at = both * both_slot + (1 - both) * 2, both * (both_at + 2) + (1 - both) * n
        else:
            both, two = (1 - odd) * (1 - upper), (1 - odd) * upper
            slot = both * both_slot + two * 2 + odd * (SIDE - off)
            at = both * (both_at + 2) + (1 - both) * n
        project(slot, at)
        return carry

    for turn in range(3):
        if turn == 1:
            with jax.named_scope("slot"):
                pltpu.make_async_copy(weights.at[2], weights.at[2], w2_recv.at[2]).wait()
        with jax.named_scope("project"):
            lax.fori_loop(0, SIDE, functools.partial(third, turn), 0)

    query = queries[...].astype(BF16)

    def score(pair, carry):
        for i in range(2):
            at = pair * 2 + i
            block = key_out.at[0, pl.ds(pl.multiple_of(at * PAIR, PAIR), PAIR)]
            pltpu.make_async_copy(block, block, kv_recv.at[0, at]).wait()
        for i in range(3):
            chunk = pair * 3 + i
            keys = key_out[0, pl.ds(pl.multiple_of(chunk * HD, HD), HD), :]
            scores[chunk] = lax.dot_general(query, keys, (((1,), (1,)), ((), ())), preferred_element_type=F32)[:8]
        return carry

    with jax.named_scope("score"):
        lax.fori_loop(0, Z // 2, score, 0)

    row = lax.broadcasted_iota(jnp.int32, (1, 8, HD), 1)
    bias = jnp.where(row % 2 == 0, bias_ref[group * 2], bias_ref[group * 2 + 1])
    score_all = scores[...] * (HD ** -0.5) + bias
    soft = log1p_unit(jnp.exp(-jnp.abs(score_all)))
    log_keep = -(jnp.maximum(score_all, 0.0) + soft)
    log_take = -(jnp.maximum(-score_all, 0.0) + soft)
    later = (
        lax.broadcasted_iota(jnp.int32, (HD, HD), 0) > lax.broadcasted_iota(jnp.int32, (HD, HD), 1)
    ).astype(F32)
    after = jnp.dot(
        log_keep.reshape(CHUNKS * 8, HD), later, preferred_element_type=F32, precision=lax.Precision.HIGHEST
    ).reshape(CHUNKS, 8, HD)
    totals = jnp.sum(log_keep, axis=2, keepdims=True)
    carried = jnp.zeros((8, 1), F32)
    for chunk in reversed(range(CHUNKS)):
        scores[chunk] = jnp.exp(log_take[chunk] + after[chunk] + carried)
        carried = carried + totals[chunk]

    def read_pair(pair, partial):
        for i in range(2):
            at = pair * 2 + i
            block = value_out.at[0, pl.ds(pl.multiple_of(at * PAIR, PAIR), PAIR)]
            pltpu.make_async_copy(block, block, kv_recv.at[1, at]).wait()
        for i in range(3):
            chunk = pair * 3 + i
            values = value_out[0, pl.ds(pl.multiple_of(chunk * HD, HD), HD), :]
            partial = partial + jnp.dot(scores[chunk].astype(BF16), values, preferred_element_type=F32)
        return partial

    with jax.named_scope("arrive"):
        partial = lax.fori_loop(0, Z // 2, read_pair, jnp.zeros((8, HD), F32))

    parts[sp] = jnp.where(row[0] < 2, partial, carried)

    def share(i, carry):
        pltpu.make_async_remote_copy(
            parts.at[sp], parts.at[sp], p_send, p_recv,
            device_id=((sp + i) % (SIDE * SIDE), tp), device_id_type=MESH,
        ).start()
        return carry

    lax.fori_loop(1, SIDE * SIDE, share, 0)
    others = parts.at[pl.ds(0, SIDE * SIDE - 1)]
    with jax.named_scope("others"):
        pltpu.make_async_copy(others, others, p_recv).wait()
    column = weights.at[0, pl.ds(0, 2 * Z - 1), 0]
    pltpu.make_async_copy(column, column, wz_send).wait()
    pltpu.make_async_copy(three, three, w1_send).wait()
    pltpu.make_async_copy(weights.at[pl.ds(0, 3)], weights.at[pl.ds(0, 3)], w2_send).wait()
    pltpu.make_async_copy(half, half, x_send).wait()

    sent = sendbuf.at[pl.ds(0, 2 * Z - 1)]
    with jax.named_scope("drain"):
        pltpu.make_async_copy(sent, sent, kv_send).wait()
    pltpu.make_async_copy(others, others, p_send).wait()


def write_out(key_ref, value_ref, parts_ref, key_out, value_out, read_out, read, sems):
    copies = [
        pltpu.make_async_copy(ref.at[0, pl.ds(i * (SPAN // 4), SPAN // 4)], out.at[0, pl.ds(i * (SPAN // 4), SPAN // 4)], sems.at[n, i])
        for n, (ref, out) in enumerate(((key_ref, key_out), (value_ref, value_out)))
        for i in range(4)
    ]
    for copy in copies:
        copy.start()
    total = jnp.zeros((2, HD), F32)
    log_later = jnp.zeros((2, HD), F32)
    for span in reversed(range(SIDE * SIDE)):
        total = total + jnp.exp(log_later) * parts_ref[span, pl.ds(0, 2), :]
        log_later = log_later + parts_ref[span, pl.ds(2, 2), :]
    read[:, pl.ds(0, HD)] = total[0:1]
    read[:, pl.ds(HD, HD)] = total[1:2]
    last = pltpu.make_async_copy(read, read_out, sems.at[2, 0])
    last.start()
    for copy in copies:
        copy.wait()
    last.wait()


def shards(tokens, in_gain, w_key, w_value, k_gain, new_query, q_gain, stick_bias):
    vmem = pl.BlockSpec(memory_space=pltpu.VMEM)
    hbm = pl.BlockSpec(memory_space=pltpu.HBM)
    dma = pltpu.SemaphoreType.DMA
    key_rows, value_rows, parts = pl.pallas_call(
        kernel,
        out_shape=(
            jax.ShapeDtypeStruct((1, SPAN, HD), BF16),
            jax.ShapeDtypeStruct((1, SPAN, HD), BF16),
            jax.ShapeDtypeStruct((SIDE * SIDE, 8, HD), F32),
        ),
        in_specs=[hbm] * 8,
        out_specs=(vmem, vmem, vmem),
        scratch_shapes=[
            pltpu.VMEM((1, D), F32),
            pltpu.VMEM(w_key.shape, BF16),
            pltpu.VMEM(w_value.shape, BF16),
            pltpu.VMEM((1, HD), F32),
            pltpu.VMEM(new_query.shape, BF16),
            pltpu.VMEM((1, HD), F32),
            pltpu.SMEM(stick_bias.shape, F32),
            pltpu.VMEM((SEQS, TOK, D), BF16),
            pltpu.VMEM((SEQS, 2, TOK, D), BF16),
            pltpu.VMEM((SIDE, 2 * Z, 4, 16, HD), BF16),
            pltpu.VMEM((2 * Z, PAIR, HD), BF16),
            pltpu.VMEM((CHUNKS, 8, HD), F32),
            pltpu.VMEM((16, HD), F32),
            pltpu.VMEM((8, SEQS, HD), F32),
            dma((7,)), dma((SEQS,)), dma, dma((Z,)), dma, dma, dma, dma, dma((SIDE,)), dma, dma,
            dma, dma((2, Z)), dma, dma,
        ],
        compiler_params=pltpu.CompilerParams(
            collective_id=0, has_side_effects=True, vmem_limit_bytes=40 * 2**20
        ),
    )(
        *(
            pltpu.with_memory_space_constraint(a, pltpu.HBM)
            for a in (
                tokens, in_gain.reshape(1, D), w_key, w_value, k_gain.reshape(1, HD), new_query,
                q_gain.reshape(1, HD), stick_bias,
            )
        )
    )
    return pl.pallas_call(
        write_out,
        out_shape=(
            jax.ShapeDtypeStruct((1, SPAN, HD), BF16),
            jax.ShapeDtypeStruct((1, SPAN, HD), BF16),
            jax.ShapeDtypeStruct((1, 2 * HD), F32),
        ),
        in_specs=[vmem] * 3,
        out_specs=[hbm] * 3,
        scratch_shapes=[pltpu.VMEM((1, 2 * HD), F32), dma((3, 4))],
        compiler_params=pltpu.CompilerParams(vmem_limit_bytes=40 * 2**20),
    )(key_rows, value_rows, parts)


def solution(mesh):
    return jax.shard_map(
        shards,
        mesh=mesh,
        in_specs=(
            P(None, ("sp", "tp"), None), P(), P("tp", None), P("tp", None), P(), P(), P(), P(),
        ),
        out_specs=(P("tp", "sp", None), P("tp", "sp", None), P("tp", None)),
        check_vma=False,
    )
```
